1024 devices in a mesh: sp: 128 (over z, y), tp: 8 (over x, core).
Axes of the slice: x: 4, y: 8, z: 16, core: 2. Of those that a mesh axis runs over, the one named last changes fastest.
Arguments:
- query: bfloat16 [65536, 1024], P('sp', 'tp'), may hold values from -6 to 6
- key: bfloat16 [65536, 1024], P('sp', 'tp'), may hold values from -6 to 6
- value: bfloat16 [65536, 1024], P('sp', 'tp'), may hold values from -6 to 6
- out_grad: bfloat16 [65536, 1024], P('sp', 'tp'), may hold values from -6 to 6
- query_gain: float32 [64], replicated, may hold values from 0.1 to 1.9
- key_gain: float32 [64], replicated, may hold values from 0.1 to 1.9
- rel_bias: float32 [16, 129], P('tp'), may hold values from -3 to 3
Outputs:
- query_grad: bfloat16 [65536, 1024], P('sp', 'tp')
- key_grad: bfloat16 [65536, 1024], P('sp', 'tp')
- value_grad: bfloat16 [65536, 1024], P('sp', 'tp')
- query_gain_grad: float32 [64], replicated
- key_gain_grad: float32 [64], replicated
- bias_grad: float32 [16, 129], P('tp')
The draws below stay inside these ranges and needn't reach their ends.
All inputs are finite; a program needn't handle non-finite values.
Results may differ from the reference program's by a relative error of at most 0.0095.
Values may be sent and summed in bfloat16 or wider, within the bound.
A program may use at most 32 MiB of HBM per device.

```python
import jax
import jax.numpy as jnp
from jax import lax

H = 16
HD = 64
SEG = 64
PREV = 8
CLIP = 128
TOKENS = 65536
ATT = 1024
TAPS = 129


def block_levels(stream_key, extent, shards, smallest, top_value):
    loudness = 1.0
    for dim, blocks in shards:
        heights = jax.random.uniform(jax.random.fold_in(jax.random.fold_in(stream_key, 6), dim), (blocks,), jnp.float32, smallest / len(shards), top_value / len(shards))
        loudness = loudness * jnp.repeat(jnp.exp(heights), extent[dim] // blocks).reshape((-1,) + (1,) * (len(extent) - 1 - dim))
    return loudness


def noise(key, shape, scale, bound, pieces=(), kind=jnp.bfloat16):
    gain = block_levels(key, shape, pieces, -0.22, 0.18) if pieces else 1.0
    entries = jax.random.normal(key, shape, jnp.float32) * scale * gain
    return jnp.minimum(jnp.maximum(entries, -bound), bound).astype(kind)


def setup_inputs(seed: int = 0) -> dict:
    splits = jax.random.split(jax.random.key(seed), 8)
    return {
        "query": noise(splits[0], (TOKENS, ATT), 1.0, 6.0, ((0, 128), (1, 8))),
        "key": noise(splits[1], (TOKENS, ATT), 1.0, 6.0, ((0, 128), (1, 8))),
        "value": noise(splits[2], (TOKENS, ATT), 1.0, 6.0, ((0, 128), (1, 8))),
        "out_grad": noise(splits[3], (TOKENS, ATT), 1.0, 6.0, ((0, 128), (1, 8))),
        "query_gain": jnp.clip(1.0 + 0.18 * jax.random.normal(splits[4], (HD,), jnp.float32), 0.1, 1.9),
        "key_gain": jnp.clip(1.0 + 0.18 * jax.random.normal(splits[5], (HD,), jnp.float32), 0.1, 1.9),
        "rel_bias": noise(splits[6], (H, TAPS), 0.5, 3.0, ((0, 8),), jnp.float32),
    }


epsilon = 1e-06

def normalize(head_rows, gain_vector):
    widened = head_rows.astype(jnp.float32)
    row_scale = lax.rsqrt(lax.optimization_barrier(jnp.mean(widened * widened, axis=-1, keepdims=True)) + epsilon)
    unit_rows = widened * row_scale
    return (unit_rows, row_scale, (unit_rows * gain_vector).astype(jnp.bfloat16))

def norm_backward(grad_hat, unit_rows, row_scale, gain_vector):
    grad_unit = grad_hat * gain_vector
    inner_mean = lax.optimization_barrier(jnp.mean(grad_unit * unit_rows, axis=-1, keepdims=True))
    return (row_scale * (grad_unit - unit_rows * inner_mean), lax.optimization_barrier(jnp.sum(grad_hat * unit_rows, axis=(0, 1))))

def bias_matrix(table_row, block):
    tap_count = table_row.shape[0]
    position = jnp.arange(3 * block - 1, dtype=jnp.int32)
    distance = jnp.clip(2 * block - 1 - position, 0, tap_count - 1)
    selected = distance[:, None] == jnp.arange(tap_count, dtype=jnp.int32)[None, :]
    diagonal = lax.optimization_barrier(jnp.sum(jnp.where(selected, table_row[None, :], jnp.zeros((), table_row.dtype)), axis=1))
    diagonal = jnp.concatenate([diagonal[block - 1:], jnp.zeros((1,), diagonal.dtype), diagonal[:block - 1]])
    flattened = jnp.tile(diagonal, block)[:block * (3 * block - 1)]
    return flattened.reshape(block, 3 * block - 1)[:, :2 * block]

def tap_totals(score_grad, tap_count):
    block = score_grad.shape[0]
    widened = jnp.pad(score_grad, ((0, 0), (0, block - 1)))
    flattened = jnp.pad(widened.reshape(-1), (0, block))
    columns = lax.optimization_barrier(jnp.sum(flattened.reshape(block, 3 * block), axis=0))
    near_taps = columns[block - tap_count + 2:block + 1][::-1]
    return jnp.concatenate([near_taps, (jnp.sum(columns) - jnp.sum(near_taps))[None]])

def band_mask(block):
    row_index = jnp.arange(block, dtype=jnp.int32)[:, None]
    col_index = jnp.arange(2 * block, dtype=jnp.int32)[None, :]
    return (row_index + block >= col_index) & (col_index // SEG >= row_index // SEG)

def block_gradients(query_block, key_block, value_block, grad_block, bias_block, allowed, score_scale, skip_rows):
    scores = jnp.dot(query_block, key_block.T, preferred_element_type=jnp.float32) * score_scale + bias_block
    normalizer = lax.optimization_barrier(jnp.sum(jnp.where(allowed, jnp.exp(scores), jnp.zeros((), jnp.float32)), axis=1, keepdims=True))
    log_total = jnp.log(normalizer)
    attention = jnp.where(allowed, jnp.exp(scores - log_total), jnp.zeros((), jnp.float32))
    attention_low = attention.astype(jnp.bfloat16)
    output_low = jnp.dot(attention_low, value_block, preferred_element_type=jnp.float32).astype(jnp.bfloat16)
    output_low = lax.optimization_barrier(output_low)
    row_delta = lax.optimization_barrier(jnp.sum(grad_block.astype(jnp.float32) * output_low.astype(jnp.float32), axis=1, keepdims=True))
    attention_grad = jnp.dot(grad_block, value_block.T, preferred_element_type=jnp.float32)
    score_grad = attention * (attention_grad - row_delta)
    score_low = score_grad.astype(jnp.bfloat16)
    query_part = jnp.dot(score_low, key_block, preferred_element_type=jnp.float32) * score_scale
    key_part = jnp.dot(score_low[:, skip_rows:].T, query_block, preferred_element_type=jnp.float32) * score_scale
    value_part = jnp.dot(attention_low[:, skip_rows:].T, grad_block, preferred_element_type=jnp.float32)
    tap_part = tap_totals(score_grad, bias_block.shape[0] * 0 + CLIP + 1)
    return (query_part, key_part, value_part, tap_part, log_total, row_delta)

def reference(query, key, value, out_grad, query_gain, key_gain, rel_bias):
    block = PREV * SEG
    score_scale = HD ** (-0.5)
    shape = (TOKENS, H, HD)
    query_unit, query_scale, query_hat = normalize(query.reshape(shape), query_gain)
    key_unit, key_scale, key_hat = normalize(key.reshape(shape), key_gain)
    padding = jnp.zeros((block, H, HD), jnp.bfloat16)
    key_heads = jnp.concatenate([padding, key_hat]).transpose(1, 0, 2)
    value_heads = jnp.concatenate([padding, value.reshape(shape)]).transpose(1, 0, 2)
    query_heads = query_hat.transpose(1, 0, 2)
    grad_heads = out_grad.reshape(shape).transpose(1, 0, 2)
    inside = band_mask(block)
    later = jnp.arange(2 * block, dtype=jnp.int32)[None, :] >= block
    block_count = TOKENS // block

    def per_head(items):
        query_rows, key_rows, value_rows, grad_rows, table_row = items
        bias_block = bias_matrix(table_row, block)

        def per_block(block_index):
            row_start = (block_index * block).astype(jnp.int32)
            allowed = inside & (later | (block_index > 0))
            query_block = lax.dynamic_slice_in_dim(query_rows, row_start, block, 0)
            key_block = lax.dynamic_slice_in_dim(key_rows, row_start, 2 * block, 0)
            value_block = lax.dynamic_slice_in_dim(value_rows, row_start, 2 * block, 0)
            grad_block = lax.dynamic_slice_in_dim(grad_rows, row_start, block, 0)
            results = block_gradients(query_block, key_block, value_block, grad_block, bias_block, allowed, score_scale, 0)
            return (results[0], results[1], results[2], results[3])
        query_part, key_part, value_part, tap_part = lax.map(per_block, jnp.arange(block_count, dtype=jnp.int32))
        key_sum = jnp.pad(key_part[:, :block].reshape(-1, HD), ((0, block), (0, 0))) + jnp.pad(key_part[:, block:].reshape(-1, HD), ((block, 0), (0, 0)))
        value_sum = jnp.pad(value_part[:, :block].reshape(-1, HD), ((0, block), (0, 0))) + jnp.pad(value_part[:, block:].reshape(-1, HD), ((block, 0), (0, 0)))
        return (query_part.reshape(-1, HD), key_sum[block:], value_sum[block:], lax.optimization_barrier(jnp.sum(tap_part, axis=0)))
    query_hat_grad, key_hat_grad, value_sum, bias_grad = lax.map(per_head, (query_heads, key_heads, value_heads, grad_heads, rel_bias))
    query_grad, query_gain_grad = norm_backward(query_hat_grad.transpose(1, 0, 2), query_unit, query_scale, query_gain)
    key_grad, key_gain_grad = norm_backward(key_hat_grad.transpose(1, 0, 2), key_unit, key_scale, key_gain)
    value_grad = value_sum.transpose(1, 0, 2).reshape(TOKENS, ATT)
    return (query_grad.reshape(TOKENS, ATT).astype(jnp.bfloat16), key_grad.reshape(TOKENS, ATT).astype(jnp.bfloat16), value_grad.astype(jnp.bfloat16), query_gain_grad, key_gain_grad, bias_grad)
```

```python
import functools

import jax
import jax.numpy as jnp
from jax import lax
from jax.experimental import pallas as pl
from jax.experimental.pallas import tpu as pltpu
from jax.sharding import Mesh
from jax.sharding import PartitionSpec as P

SP = ("z", "y")
TP = ("x", "c")
MESH = pl.DeviceIdType.MESH

ROWS = 512
TILE = 128
TILES = ROWS // TILE
LANES = 128
HD = 64
WIDE = 2 * TILE
EPS = 1e-06
LOG2E = 1.4426950408889634
SCALE = HD**-0.5
OFF = -1e30

f32 = jnp.float32
bf16 = jnp.bfloat16


def dot(a, b, dims=((1,), (0,))):
    return lax.dot_general(a, b, (dims, ((), ())), preferred_element_type=f32)


def iota(shape, axis):
    return lax.broadcasted_iota(jnp.int32, shape, axis)


def head_sums(x, ones):
    high = x.astype(bf16)
    low = (x - high.astype(f32)).astype(bf16)
    return dot(high, ones) + dot(low, ones)


def normalize(x, gain, ones):
    wide = x.astype(f32)
    scale = lax.rsqrt(head_sums(wide * wide, ones) * (1.0 / HD) + EPS)
    unit = wide * scale
    return unit, scale, (unit * gain).astype(bf16)


def norm_backward(grad_hat, unit, scale, gain, ones):
    grad_unit = grad_hat * gain
    inner = head_sums(grad_unit * unit, ones) * (1.0 / HD)
    return scale * (grad_unit - unit * inner)


def shifted_rows(row):
    rows = jnp.broadcast_to(row, (8, LANES))
    index = iota((8, LANES), 0)
    for bit in (1, 2, 4):
        rows = jnp.where((index & bit) != 0, pltpu.roll(rows, bit, 1), rows)
    size = 8
    while size < TILE:
        rows = jnp.concatenate([rows, pltpu.roll(rows, size, 1)], axis=0)
        size *= 2
    return rows


def diagonal_sums(block):
    size = TILE
    while size > 8:
        size //= 2
        block = block[:size] + pltpu.roll(block[size:], LANES - size, 1)
    index = iota((8, LANES), 0)
    for bit in (1, 2, 4):
        block = jnp.where((index & bit) != 0, pltpu.roll(block, LANES - bit, 1), block)
    return jnp.sum(block, axis=0, keepdims=True)


def both_heads(a):
    first = iota((TILE, LANES), 1) < HD
    zero = jnp.zeros((), a.dtype)
    return jnp.concatenate([jnp.where(first, a, zero), jnp.where(first, zero, a)], axis=0)


def body(
    sizes,
    q_ref,
    k_ref,
    v_ref,
    g_ref,
    qgain_ref,
    kgain_ref,
    bias_ref,
    dq_ref,
    dk_ref,
    dv_ref,
    dqgain_ref,
    dkgain_ref,
    dbias_ref,
    hk_ref,
    hv_ref,
    nq_ref,
    ng_ref,
    send_stat,
    recv_stat,
    unit_q,
    scale_q,
    khat_ref,
    hkhat_ref,
    qm_ref,
    gm_ref,
    qmn_ref,
    gmn_ref,
    e_ref,
    d_ref,
    en_ref,
    dn_ref,
    pown_ref,
    sown_ref,
    pn_ref,
    sn_ref,
    ybuf,
    zbuf,
    tbuf,
    halo_send,
    halo_recv,
    stat_ssem,
    stat_rsem,
    y_ssem,
    y_rsem,
    z_ssem,
    z_rsem,
    t_ssem,
    t_rsem,
):
    nz, ny, nx, nc = sizes
    nsp, ntp = nz * ny, nx * nc
    z, y, x, c = (lax.axis_index(a) for a in ("z", "y", "x", "c"))
    sp = z * ny + y
    after, before = lax.rem(sp + 1, nsp), lax.rem(sp + nsp - 1, nsp)
    t_me = x * nc + c

    def at_sp(i):
        return {"z": i // ny, "y": lax.rem(i, ny)}

    def at_tp(i):
        return {"x": i // nc, "c": lax.rem(i, nc)}

    y_peers = [lax.rem(y + d, ny) for d in range(1, ny)]
    z_peers = [lax.rem(z + d, nz) for d in range(1, nz)]
    t_peers = [lax.rem(t_me + d, ntp) for d in range(1, ntp)]

    barrier = pltpu.get_barrier_semaphore()
    targets = [at_sp(after), at_sp(before)]
    targets += [{"y": p} for p in y_peers]
    targets += [{"z": p} for p in z_peers]
    targets += [at_tp(p) for p in t_peers]
    for target in targets:
        pl.semaphore_signal(barrier, inc=1, device_id=target, device_id_type=MESH)
    pl.semaphore_wait(barrier, len(targets))

    def halo_copy(kind, tile):
        src, dst, to = (
            (k_ref, hk_ref, after),
            (v_ref, hv_ref, after),
            (q_ref, nq_ref, before),
            (g_ref, ng_ref, before),
        )[kind]
        rows = pl.ds(tile * TILE, TILE)
        return pltpu.make_async_remote_copy(
            src_ref=src.at[rows],
            dst_ref=dst.at[rows],
            send_sem=halo_send.at[kind, tile],
            recv_sem=halo_recv.at[kind, tile],
            device_id=at_sp(to),
            device_id_type=MESH,
        )

    for tile in reversed(range(TILES)):
        for kind in range(4):
            halo_copy(kind, tile).start()

    ones = (iota((LANES, LANES), 0) // HD == iota((LANES, LANES), 1) // HD).astype(bf16)
    qgain = jnp.concatenate([qgain_ref[...], qgain_ref[...]], axis=1)
    kgain = jnp.concatenate([kgain_ref[...], kgain_ref[...]], axis=1)

    key_i, query_i = iota((TILE, TILE), 0), iota((TILE, TILE), 1)
    reached = query_i >= key_i
    near, mid, far = [], [], []
    for h in range(2):
        row = bias_ref[h : h + 1, 0:LANES] * LOG2E
        last = bias_ref[h : h + 1, LANES : LANES + 1] * LOG2E
        table = shifted_rows(row)
        near.append(jnp.where(reached, table, OFF))
        mid.append(jnp.where(reached, last, table))
        far.append(jnp.broadcast_to(last, (1, TILE)))
    near = jnp.concatenate(near, axis=1)
    mid = jnp.concatenate(mid, axis=1)
    far = jnp.concatenate(far, axis=1)
    both_reached = jnp.concatenate([reached, reached], axis=1)
    wide_q = lax.rem(iota((TILE, WIDE), 1), TILE) // HD
    wide_k = iota((TILE, WIDE), 0) // HD
    edge = jnp.where(wide_k >= wide_q, 0.0, OFF)
    halo_off = jnp.where(sp > 0, 0.0, OFF)
    next_off = jnp.where(sp < nsp - 1, 0.0, OFF)

    def own_bias(distance):
        return (near, mid, far)[min(distance, 2)]

    def halo_bias(distance, off):
        if distance == 0:
            return far + edge + off
        return (mid if distance == TILES - 1 else far) + off

    for t in range(TILES):
        rows = slice(t * TILE, (t + 1) * TILE)
        unit, scale, hat = normalize(q_ref[rows], qgain, ones)
        unit_q[rows] = unit
        scale_q[rows] = scale
        qm_ref[t * WIDE : (t + 1) * WIDE] = both_heads(hat)
        gm_ref[t * WIDE : (t + 1) * WIDE] = both_heads(g_ref[rows])
    khat_ref[...] = normalize(k_ref[...], kgain, ones)[2]

    nt = ((1,), (1,))
    l_parts, n_parts = [], []
    for t in range(TILES):
        cols = slice(t * WIDE, (t + 1) * WIDE)
        count = (t + 1) * TILE
        s = dot(khat_ref[0:count], qm_ref[cols], nt)
        d = dot(v_ref[0:count], gm_ref[cols], nt)
        l_sum = jnp.zeros((1, WIDE), f32)
        n_sum = jnp.zeros((1, WIDE), f32)
        for ck in range(t + 1):
            part = slice(ck * TILE, (ck + 1) * TILE)
            slot = slice((TILES - t + ck) * TILE, (TILES - t + ck + 1) * TILE)
            e = jnp.exp2(s[part] * (SCALE * LOG2E) + own_bias(t - ck))
            e_ref[t, slot] = e
            d_ref[t, slot] = d[part]
            l_sum += jnp.sum(e, axis=0, keepdims=True)
            n_sum += jnp.sum(e * d[part], axis=0, keepdims=True)
        l_parts.append(l_sum)
        n_parts.append(n_sum)

    def stat_copy(t):
        return pltpu.make_async_remote_copy(
            src_ref=send_stat.at[t],
            dst_ref=recv_stat.at[t],
            send_sem=stat_ssem.at[t],
            recv_sem=stat_rsem.at[t],
            device_id=at_sp(before),
            device_id_type=MESH,
        )

    total = jnp.zeros((1, WIDE), f32)
    near_sum = jnp.zeros((TILE, WIDE), f32)
    mid_sum = jnp.zeros((TILE, WIDE), f32)
    gain_sum = jnp.zeros((1, LANES), f32)
    for ck in reversed(range(TILES)):
        rows = slice(ck * TILE, (ck + 1) * TILE)
        halo_copy(0, ck).wait_recv()
        hkhat_ref[rows] = normalize(hk_ref[rows], kgain, ones)[2]
        halo_copy(1, ck).wait_recv()
        span = (ck + 1) * WIDE
        s = dot(hkhat_ref[rows], qm_ref[0:span], nt)
        d = dot(hv_ref[rows], gm_ref[0:span], nt)
        for t in range(ck + 1):
            part = slice(t * WIDE, (t + 1) * WIDE)
            slot = slice((ck - t) * TILE, (ck - t + 1) * TILE)
            e = jnp.exp2(s[:, part] * (SCALE * LOG2E) + halo_bias(ck - t, halo_off))
            e_ref[t, slot] = e
            d_ref[t, slot] = d[:, part]
            l_parts[t] += jnp.sum(e, axis=0, keepdims=True)
            n_parts[t] += jnp.sum(e * d[:, part], axis=0, keepdims=True)
        t = ck
        inv = 1.0 / l_parts[t]
        delta = n_parts[t] * inv
        send_stat[t, 0:1] = inv
        send_stat[t, 1:2] = delta
        stat_copy(t).start()
        cols = slice(t * WIDE, (t + 1) * WIDE)
        prob = e_ref[t] * inv
        grad = prob * (d_ref[t] - delta)
        total += jnp.sum(grad, axis=0, keepdims=True)
        own = (TILES - t) * TILE
        near_sum += grad[TILES * TILE :]
        if t > 0:
            mid_sum += grad[(TILES - 1) * TILE : TILES * TILE]
        else:
            mid_sum += grad[(TILES - 1) * TILE : TILES * TILE]
        low = grad.astype(bf16)
        pown_ref[0 : (t + 1) * TILE, cols] = prob[own:].astype(bf16)
        sown_ref[0 : (t + 1) * TILE, cols] = low[own:]
        keys = jnp.concatenate([hkhat_ref[t * TILE :], khat_ref[0 : (t + 1) * TILE]], axis=0)
        dq_t = dot(keys, low, ((0,), (0,)))
        dq_t = jnp.concatenate([dq_t[0:HD, 0:TILE], dq_t[HD:, TILE:]], axis=0) * SCALE
        grad_hat = dq_t.T
        unit = unit_q[rows]
        gain_sum += jnp.sum(grad_hat * unit, axis=0, keepdims=True)
        dq_ref[rows] = norm_backward(grad_hat, unit, scale_q[rows], qgain, ones).astype(bf16)

    diagonals = jnp.where(both_reached, near_sum, mid_sum)
    taps = [diagonal_sums(diagonals[:, h * TILE : (h + 1) * TILE]) for h in range(2)]
    sums = [jnp.sum(total[:, h * TILE : (h + 1) * TILE], axis=1, keepdims=True) for h in range(2)]
    lane = iota((1, LANES), 1)
    sums = jnp.where(lane < HD, sums[0], sums[1])
    ybuf[y] = jnp.concatenate([taps[0], taps[1], gain_sum, sums], axis=0)

    def y_copy(peer, slot):
        return pltpu.make_async_remote_copy(
            src_ref=ybuf.at[slot],
            dst_ref=ybuf.at[slot],
            send_sem=y_ssem.at[peer],
            recv_sem=y_rsem.at[slot],
            device_id={"y": peer},
            device_id_type=MESH,
        )

    def z_copy(peer, slot):
        return pltpu.make_async_remote_copy(
            src_ref=zbuf.at[slot],
            dst_ref=zbuf.at[slot],
            send_sem=z_ssem.at[peer],
            recv_sem=z_rsem.at[slot],
            device_id={"z": peer},
            device_id_type=MESH,
        )

    def t_copy(peer, slot):
        return pltpu.make_async_remote_copy(
            src_ref=tbuf.at[slot],
            dst_ref=tbuf.at[slot],
            send_sem=t_ssem.at[peer],
            recv_sem=t_rsem.at[slot],
            device_id=at_tp(peer),
            device_id_type=MESH,
        )

    for p in y_peers:
        y_copy(p, y).start()

    for t in reversed(range(TILES)):
        rows = slice(t * TILE, (t + 1) * TILE)
        cols = slice(t * WIDE, (t + 1) * WIDE)
        halo_copy(2, t).wait_recv()
        qmn_ref[cols] = both_heads(normalize(nq_ref[rows], qgain, ones)[2])
        halo_copy(3, t).wait_recv()
        gmn_ref[cols] = both_heads(ng_ref[rows])
        s = dot(khat_ref[t * TILE :], qmn_ref[cols], nt)
        d = dot(v_ref[t * TILE :], gmn_ref[cols], nt)
        for ck in range(t, TILES):
            part = slice((ck - t) * TILE, (ck - t + 1) * TILE)
            rows = slice(ck * TILE, (ck + 1) * TILE)
            en_ref[rows, cols] = jnp.exp2(
                s[part] * (SCALE * LOG2E) + halo_bias(ck - t, next_off)
            )
            dn_ref[rows, cols] = d[part]

    for p in y_peers:
        y_copy(p, p).wait_recv()
    summed = ybuf[0]
    for i in range(1, ny):
        summed += ybuf[i]
    zbuf[z] = summed
    for p in z_peers:
        z_copy(p, z).start()

    for t in reversed(range(TILES)):
        cols = slice(t * WIDE, (t + 1) * WIDE)
        stat_copy(t).wait_recv()
        inv, delta = recv_stat[t, 0:1], recv_stat[t, 1:2]
        prob = en_ref[t * TILE :, cols] * inv
        pn_ref[t * TILE :, cols] = prob.astype(bf16)
        sn_ref[t * TILE :, cols] = (prob * (dn_ref[t * TILE :, cols] - delta)).astype(bf16)

    unit_k, scale_k, _ = normalize(k_ref[...], kgain, ones)
    for ck in range(TILES):
        rows = slice(ck * TILE, (ck + 1) * TILE)
        own, later = slice(ck * WIDE, TILES * WIDE), slice(0, (ck + 1) * WIDE)
        dv = dot(pown_ref[rows, own], gm_ref[own]) + dot(pn_ref[rows, later], gmn_ref[later])
        dv_ref[rows] = dv.astype(bf16)
        dk = dot(sown_ref[rows, own], qm_ref[own]) + dot(sn_ref[rows, later], qmn_ref[later])
        dk_ref[rows] = norm_backward(
            dk * SCALE, unit_k[rows], scale_k[rows], kgain, ones
        ).astype(bf16)

    for p in z_peers:
        z_copy(p, p).wait_recv()
    summed = zbuf[0]
    for i in range(1, nz):
        summed += zbuf[i]
    tbuf[t_me] = summed[2:3]
    for p in t_peers:
        t_copy(p, t_me).start()
    rest = [summed[3:4, h * HD : h * HD + 1] for h in range(2)]
    for h in range(2):
        taps = summed[h : h + 1]
        dbias_ref[h : h + 1, 0:LANES] = taps
        dbias_ref[h : h + 1, LANES : LANES + 1] = rest[h] - jnp.sum(taps, axis=1, keepdims=True)

    for p in t_peers:
        t_copy(p, p).wait_recv()
    summed = tbuf[0]
    for i in range(1, ntp):
        summed += tbuf[i]
    summed = (summed + pltpu.roll(summed, HD, 1))[:, 0:HD]
    dqgain_ref[...] = summed
    dkgain_ref[...] = summed * qgain_ref[...] / kgain_ref[...]

    for tile in range(TILES):
        for kind in range(4):
            halo_copy(kind, tile).wait_send()
        stat_copy(tile).wait_send()
    for p in y_peers:
        y_copy(p, y).wait_send()
    for p in z_peers:
        z_copy(p, z).wait_send()
    for p in t_peers:
        t_copy(p, t_me).wait_send()


def per_device(sizes, query, key, value, out_grad, query_gain, key_gain, rel_bias):
    nz, ny, nx, nc = sizes
    vmem = pl.BlockSpec(memory_space=pltpu.VMEM)
    dma = pltpu.SemaphoreType.DMA
    big = jax.ShapeDtypeStruct((ROWS, LANES), bf16)
    gain = jax.ShapeDtypeStruct((1, HD), f32)
    outs = pl.pallas_call(
        functools.partial(body, sizes),
        out_shape=(big, big, big, gain, gain, jax.ShapeDtypeStruct(rel_bias.shape, f32)),
        in_specs=[vmem] * 7,
        out_specs=(vmem,) * 6,
        scratch_shapes=[
            pltpu.VMEM((ROWS, LANES), bf16),
            pltpu.VMEM((ROWS, LANES), bf16),
            pltpu.VMEM((ROWS, LANES), bf16),
            pltpu.VMEM((ROWS, LANES), bf16),
            pltpu.VMEM((TILES, 8, WIDE), f32),
            pltpu.VMEM((TILES, 8, WIDE), f32),
            pltpu.VMEM((ROWS, LANES), f32),
            pltpu.VMEM((ROWS, LANES), f32),
            pltpu.VMEM((ROWS, LANES), bf16),
            pltpu.VMEM((ROWS, LANES), bf16),
            pltpu.VMEM((TILES * WIDE, LANES), bf16),
            pltpu.VMEM((TILES * WIDE, LANES), bf16),
            pltpu.VMEM((TILES * WIDE, LANES), bf16),
            pltpu.VMEM((TILES * WIDE, LANES), bf16),
            pltpu.VMEM((TILES, (TILES + 1) * TILE, WIDE), f32),
            pltpu.VMEM((TILES, (TILES + 1) * TILE, WIDE), f32),
            pltpu.VMEM((ROWS, TILES * WIDE), f32),
            pltpu.VMEM((ROWS, TILES * WIDE), f32),
            pltpu.VMEM((ROWS, TILES * WIDE), bf16),
            pltpu.VMEM((ROWS, TILES * WIDE), bf16),
            pltpu.VMEM((ROWS, TILES * WIDE), bf16),
            pltpu.VMEM((ROWS, TILES * WIDE), bf16),
            pltpu.VMEM((ny, 4, LANES), f32),
            pltpu.VMEM((nz, 4, LANES), f32),
            pltpu.VMEM((nx * nc, 1, LANES), f32),
            dma((4, TILES)),
            dma((4, TILES)),
            dma((TILES,)),
            dma((TILES,)),
            dma((ny,)),
            dma((ny,)),
            dma((nz,)),
            dma((nz,)),
            dma((nx * nc,)),
            dma((nx * nc,)),
        ],
        compiler_params=pltpu.CompilerParams(collective_id=0, has_side_effects=True),
        name="segment_backward",
    )(query, key, value, out_grad, query_gain.reshape(1, HD), key_gain.reshape(1, HD), rel_bias)
    return (*outs[:3], outs[3].reshape(HD), outs[4].reshape(HD), outs[5])


def solution(mesh):
    sizes = mesh_sizes(mesh)
    torus = Mesh(mesh.devices.reshape(sizes), ("z", "y", "x", "c"))
    return jax.shard_map(
        functools.partial(per_device, sizes),
        mesh=torus,
        in_specs=(P(SP, TP), P(SP, TP), P(SP, TP), P(SP, TP), P(), P(), P(TP, None)),
        out_specs=(P(SP, TP), P(SP, TP), P(SP, TP), P(), P(), P(TP, None)),
        check_vma=False,
    )


def mesh_sizes(mesh):
    return (16, 8, 4, 2)
```

```python
import functools

import jax
import jax.numpy as jnp
from jax import lax
from jax.experimental import pallas as pl
from jax.experimental.pallas import tpu as pltpu
from jax.sharding import Mesh
from jax.sharding import PartitionSpec as P

SP = ("z", "y")
TP = ("x", "c")
MESH = pl.DeviceIdType.MESH

ROWS = 512
TILE = 128
TILES = ROWS // TILE
LANES = 128
HD = 64
WIDE = 2 * TILE
EPS = 1e-06
LOG2E = 1.4426950408889634
SCALE = HD**-0.5
OFF = -1e30

f32 = jnp.float32
bf16 = jnp.bfloat16


def dot(a, b, dims=((1,), (0,))):
    return lax.dot_general(a, b, (dims, ((), ())), preferred_element_type=f32)


def iota(shape, axis):
    return lax.broadcasted_iota(jnp.int32, shape, axis)


def head_sums(x, ones):
    high = x.astype(bf16)
    low = (x - high.astype(f32)).astype(bf16)
    return dot(high, ones) + dot(low, ones)


def normalize(x, gain, ones):
    wide = x.astype(f32)
    scale = lax.rsqrt(head_sums(wide * wide, ones) * (1.0 / HD) + EPS)
    unit = wide * scale
    return unit, scale, (unit * gain).astype(bf16)


def norm_backward(grad_hat, unit, scale, gain, ones):
    grad_unit = grad_hat * gain
    inner = head_sums(grad_unit * unit, ones) * (1.0 / HD)
    return scale * (grad_unit - unit * inner)


def shifted_rows(row):
    rows = jnp.broadcast_to(row, (8, LANES))
    index = iota((8, LANES), 0)
    for bit in (1, 2, 4):
        rows = jnp.where((index & bit) != 0, pltpu.roll(rows, bit, 1), rows)
    size = 8
    while size < TILE:
        rows = jnp.concatenate([rows, pltpu.roll(rows, size, 1)], axis=0)
        size *= 2
    return rows


def diagonal_sums(block):
    size = TILE
    while size > 8:
        size //= 2
        block = block[:size] + pltpu.roll(block[size:], LANES - size, 1)
    index = iota((8, LANES), 0)
    for bit in (1, 2, 4):
        block = jnp.where((index & bit) != 0, pltpu.roll(block, LANES - bit, 1), block)
    return jnp.sum(block, axis=0, keepdims=True)


def both_heads(a):
    first = iota((TILE, LANES), 1) < HD
    zero = jnp.zeros((), a.dtype)
    return jnp.concatenate([jnp.where(first, a, zero), jnp.where(first, zero, a)], axis=0)


def body(
    sizes,
    q_hbm,
    k_hbm,
    v_hbm,
    g_hbm,
    qgain_hbm,
    kgain_hbm,
    bias_hbm,
    dq_ref,
    dk_ref,
    dv_ref,
    dqgain_ref,
    dkgain_ref,
    dbias_ref,
    q_ref,
    k_ref,
    v_ref,
    g_ref,
    qgain_ref,
    kgain_ref,
    bias_ref,
    hk_ref,
    hv_ref,
    nq_ref,
    ng_ref,
    send_stat,
    recv_stat,
    unit_q,
    scale_q,
    grad_q,
    khat_ref,
    hkhat_ref,
    qm_ref,
    gm_ref,
    qmn_ref,
    gmn_ref,
    e_ref,
    d_ref,
    en_ref,
    dn_ref,
    pown_ref,
    sown_ref,
    pn_ref,
    sn_ref,
    abuf,
    again,
    asend,
    bbuf,
    bgain,
    bsend,
    load_sem,
    halo_send,
    halo_recv,
    stat_ssem,
    stat_rsem,
    a_ssem,
    a_rsem,
    b_ssem,
    b_rsem,
    level_1,
    level_2,
    level_3,
    x_ready,
    c_ready,
):
    nz, ny, nx, nc = sizes
    nsp = nz * ny
    z, y, x, c = (lax.axis_index(a) for a in ("z", "y", "x", "c"))
    sp = z * ny + y
    after, before = lax.rem(sp + 1, nsp), lax.rem(sp + nsp - 1, nsp)

    def at_sp(i):
        return {"z": i // ny, "y": lax.rem(i, ny)}

    def both_ways(name, place, size, distance):
        return [
            {name: lax.rem(place + distance, size)},
            {name: lax.rem(place + (distance // size + 1) * size - distance, size)},
        ]

    def tell(sem, targets):
        for target in targets:
            pl.semaphore_signal(sem, inc=1, device_id=target, device_id_type=MESH)

    axes = both_ways("z", z, nz, 1) + both_ways("y", y, ny, 1)
    if nx > 1:
        axes += both_ways("x", x, nx, 1)
    partner = [{"c": lax.rem(c + d, nc)} for d in range(1, nc)]
    x_peers = [{"x": lax.rem(x + d, nx)} for d in range(1, nx)]
    two_away = both_ways("z", z, nz, 2) + both_ways("y", y, ny, 2)
    four_away = both_ways("z", z, nz, 4)

    barrier = pltpu.get_barrier_semaphore()
    neighbours = [at_sp(after), at_sp(before)] + axes + partner
    tell(barrier, neighbours)

    loads = [
        pltpu.make_async_copy(src, dst, load_sem.at[i])
        for i, (src, dst) in enumerate(
            (
                (k_hbm, k_ref),
                (v_hbm, v_ref),
                (q_hbm, q_ref),
                (g_hbm, g_ref),
                (qgain_hbm, qgain_ref),
                (kgain_hbm, kgain_ref),
                (bias_hbm, bias_ref),
            )
        )
    ]
    for load in loads:
        load.start()
    pl.semaphore_wait(barrier, len(neighbours))
    tell(level_1, axes)
    for load in loads:
        load.wait()

    def halo_copy(kind, tile):
        src, dst, to = (
            (k_ref, hk_ref, after),
            (v_ref, hv_ref, after),
            (q_ref, nq_ref, before),
            (g_ref, ng_ref, before),
        )[kind]
        rows = pl.ds(tile * TILE, TILE)
        return pltpu.make_async_remote_copy(
            src_ref=src.at[rows],
            dst_ref=dst.at[rows],
            send_sem=halo_send.at[kind, tile],
            recv_sem=halo_recv.at[kind, tile],
            device_id=at_sp(to),
            device_id_type=MESH,
        )

    for tile in reversed(range(TILES)):
        for kind in range(4):
            halo_copy(kind, tile).start()

    ones = (iota((LANES, LANES), 0) // HD == iota((LANES, LANES), 1) // HD).astype(bf16)
    qgain = jnp.concatenate([qgain_ref[...], qgain_ref[...]], axis=1)
    kgain = jnp.concatenate([kgain_ref[...], kgain_ref[...]], axis=1)

    key_i, query_i = iota((TILE, TILE), 0), iota((TILE, TILE), 1)
    reached = query_i >= key_i
    near, mid, far = [], [], []
    for h in range(2):
        row = bias_ref[h : h + 1, 0:LANES] * LOG2E
        last = bias_ref[h : h + 1, LANES : LANES + 1] * LOG2E
        table = shifted_rows(row)
        near.append(jnp.where(reached, table, OFF))
        mid.append(jnp.where(reached, last, table))
        far.append(jnp.broadcast_to(last, (1, TILE)))
    near = jnp.concatenate(near, axis=1)
    mid = jnp.concatenate(mid, axis=1)
    far = jnp.concatenate(far, axis=1)
    both_reached = jnp.concatenate([reached, reached], axis=1)
    wide_q = lax.rem(iota((TILE, WIDE), 1), TILE) // HD
    wide_k = iota((TILE, WIDE), 0) // HD
    edge = jnp.where(wide_k >= wide_q, 0.0, OFF)
    halo_off = jnp.where(sp > 0, 0.0, OFF)
    next_off = jnp.where(sp < nsp - 1, 0.0, OFF)

    def own_bias(distance):
        return (near, mid, far)[min(distance, 2)]

    def halo_bias(distance, off):
        if distance == 0:
            return far + edge + off
        return (mid if distance == TILES - 1 else far) + off

    for t in range(TILES):
        rows = slice(t * TILE, (t + 1) * TILE)
        unit, scale, hat = normalize(q_ref[rows], qgain, ones)
        unit_q[rows] = unit
        scale_q[rows] = scale
        qm_ref[t * WIDE : (t + 1) * WIDE] = both_heads(hat)
        gm_ref[t * WIDE : (t + 1) * WIDE] = both_heads(g_ref[rows])
    khat_ref[...] = normalize(k_ref[...], kgain, ones)[2]
    pl.semaphore_wait(level_1, len(axes))
    tell(level_2, two_away)

    nt = ((1,), (1,))
    l_parts, n_parts = [], []
    for t in range(TILES):
        cols = slice(t * WIDE, (t + 1) * WIDE)
        count = (t + 1) * TILE
        s = dot(khat_ref[0:count], qm_ref[cols], nt)
        d = dot(v_ref[0:count], gm_ref[cols], nt)
        l_sum = jnp.zeros((1, WIDE), f32)
        n_sum = jnp.zeros((1, WIDE), f32)
        for ck in range(t + 1):
            part = slice(ck * TILE, (ck + 1) * TILE)
            slot = slice((TILES - t + ck) * TILE, (TILES - t + ck + 1) * TILE)
            e = jnp.exp2(s[part] * (SCALE * LOG2E) + own_bias(t - ck))
            e_ref[t, slot] = e
            d_ref[t, slot] = d[part]
            l_sum += jnp.sum(e, axis=0, keepdims=True)
            n_sum += jnp.sum(e * d[part], axis=0, keepdims=True)
        l_parts.append(l_sum)
        n_parts.append(n_sum)
    pl.semaphore_wait(level_2, len(two_away))
    tell(level_3, four_away)
    tell(x_ready, x_peers)

    def stat_copy(t):
        return pltpu.make_async_remote_copy(
            src_ref=send_stat.at[t],
            dst_ref=recv_stat.at[t],
            send_sem=stat_ssem.at[t],
            recv_sem=stat_rsem.at[t],
            device_id=at_sp(before),
            device_id_type=MESH,
        )

    total = jnp.zeros((1, WIDE), f32)
    near_sum = jnp.zeros((TILE, WIDE), f32)
    mid_sum = jnp.zeros((TILE, WIDE), f32)
    gain_sum = jnp.zeros((1, LANES), f32)
    for ck in reversed(range(TILES)):
        rows = slice(ck * TILE, (ck + 1) * TILE)
        halo_copy(0, ck).wait_recv()
        hkhat_ref[rows] = normalize(hk_ref[rows], kgain, ones)[2]
        halo_copy(1, ck).wait_recv()
        span = (ck + 1) * WIDE
        s = dot(hkhat_ref[rows], qm_ref[0:span], nt)
        d = dot(hv_ref[rows], gm_ref[0:span], nt)
        for t in range(ck + 1):
            part = slice(t * WIDE, (t + 1) * WIDE)
            slot = slice((ck - t) * TILE, (ck - t + 1) * TILE)
            e = jnp.exp2(s[:, part] * (SCALE * LOG2E) + halo_bias(ck - t, halo_off))
            e_ref[t, slot] = e
            d_ref[t, slot] = d[:, part]
            l_parts[t] += jnp.sum(e, axis=0, keepdims=True)
            n_parts[t] += jnp.sum(e * d[:, part], axis=0, keepdims=True)
        t = ck
        inv = 1.0 / l_parts[t]
        delta = n_parts[t] * inv
        send_stat[t, 0:1] = inv
        send_stat[t, 1:2] = delta
        stat_copy(t).start()
        cols = slice(t * WIDE, (t + 1) * WIDE)
        prob = e_ref[t] * inv
        grad = prob * (d_ref[t] - delta)
        total += jnp.sum(grad, axis=0, keepdims=True)
        own = (TILES - t) * TILE
        near_sum += grad[TILES * TILE :]
        mid_sum += grad[(TILES - 1) * TILE : TILES * TILE]
        low = grad.astype(bf16)
        pown_ref[0 : (t + 1) * TILE, cols] = prob[own:].astype(bf16)
        sown_ref[0 : (t + 1) * TILE, cols] = low[own:]
        keys = jnp.concatenate([hkhat_ref[t * TILE :], khat_ref[0 : (t + 1) * TILE]], axis=0)
        dq_t = dot(keys, low, ((0,), (0,)))
        dq_t = jnp.concatenate([dq_t[0:HD, 0:TILE], dq_t[HD:, TILE:]], axis=0) * SCALE
        grad_hat = dq_t.T
        grad_q[rows] = grad_hat
        gain_sum += jnp.sum(grad_hat * unit_q[rows], axis=0, keepdims=True)

    diagonals = jnp.where(both_reached, near_sum, mid_sum)
    taps = [diagonal_sums(diagonals[:, h * TILE : (h + 1) * TILE]) for h in range(2)]
    sums = [jnp.sum(total[:, h * TILE : (h + 1) * TILE], axis=1, keepdims=True) for h in range(2)]
    lane = iota((1, LANES), 1)
    sums = jnp.where(lane < HD, sums[0], sums[1])
    abuf[y] = jnp.concatenate([taps[0], taps[1], sums, gain_sum], axis=0)
    asend[...] = gain_sum

    a_offsets = [(dy, dx) for dx in range(nx) for dy in range(ny) if (dy, dx) != (0, 0)]

    def a_copy(dy, dx, arriving=False):
        to_y, to_x = lax.rem(y + dy, ny), lax.rem(x + dx, nx)
        source_y, source_x = (to_y, to_x) if arriving else (y, x)
        slot = source_x * ny + source_y
        return pltpu.make_async_remote_copy(
            src_ref=abuf.at[source_y] if dx == 0 else asend,
            dst_ref=abuf.at[source_y] if dx == 0 else again.at[slot],
            send_sem=a_ssem.at[to_x * ny + to_y],
            recv_sem=a_rsem.at[slot],
            device_id={"y": to_y, "x": to_x},
            device_id_type=MESH,
        )

    if x_peers:
        pl.semaphore_wait(x_ready, len(x_peers))
    for dy, dx in a_offsets:
        a_copy(dy, dx).start()
    pl.semaphore_wait(level_3, len(four_away))
    tell(c_ready, partner)

    for t in reversed(range(TILES)):
        rows = slice(t * TILE, (t + 1) * TILE)
        cols = slice(t * WIDE, (t + 1) * WIDE)
        halo_copy(2, t).wait_recv()
        qmn_ref[cols] = both_heads(normalize(nq_ref[rows], qgain, ones)[2])
        halo_copy(3, t).wait_recv()
        gmn_ref[cols] = both_heads(ng_ref[rows])
        s = dot(khat_ref[t * TILE :], qmn_ref[cols], nt)
        d = dot(v_ref[t * TILE :], gmn_ref[cols], nt)
        for ck in range(t, TILES):
            part = slice((ck - t) * TILE, (ck - t + 1) * TILE)
            rows = slice(ck * TILE, (ck + 1) * TILE)
            en_ref[rows, cols] = jnp.exp2(
                s[part] * (SCALE * LOG2E) + halo_bias(ck - t, next_off)
            )
            dn_ref[rows, cols] = d[part]

    for dy, dx in a_offsets:
        a_copy(dy, dx, arriving=True).wait_recv()
    block = abuf[0]
    for i in range(1, ny):
        block += abuf[i]
    for i in range(ny):
        again[x * ny + i] = abuf[i, 3:4]
    gain_sum = again[0]
    for i in range(1, nx * ny):
        gain_sum += again[i]
    bbuf[z] = jnp.concatenate([block[0:3], gain_sum], axis=0)
    bsend[...] = gain_sum

    b_offsets = [(dz, dc) for dc in range(nc) for dz in range(nz) if (dz, dc) != (0, 0)]

    def b_copy(dz, dc, arriving=False):
        to_z, to_c = lax.rem(z + dz, nz), lax.rem(c + dc, nc)
        source_z, source_c = (to_z, to_c) if arriving else (z, c)
        slot = source_c * nz + source_z
        return pltpu.make_async_remote_copy(
            src_ref=bbuf.at[source_z] if dc == 0 else bsend,
            dst_ref=bbuf.at[source_z] if dc == 0 else bgain.at[slot],
            send_sem=b_ssem.at[to_c * nz + to_z],
            recv_sem=b_rsem.at[slot],
            device_id={"z": to_z, "c": to_c},
            device_id_type=MESH,
        )

    if partner:
        pl.semaphore_wait(c_ready, len(partner))
    for dz, dc in b_offsets:
        b_copy(dz, dc).start()

    for t in reversed(range(TILES)):
        rows = slice(t * TILE, (t + 1) * TILE)
        cols = slice(t * WIDE, (t + 1) * WIDE)
        stat_copy(t).wait_recv()
        inv, delta = recv_stat[t, 0:1], recv_stat[t, 1:2]
        prob = en_ref[t * TILE :, cols] * inv
        pn_ref[t * TILE :, cols] = prob.astype(bf16)
        sn_ref[t * TILE :, cols] = (prob * (dn_ref[t * TILE :, cols] - delta)).astype(bf16)
        dq_ref[rows] = norm_backward(
            grad_q[rows], unit_q[rows], scale_q[rows], qgain, ones
        ).astype(bf16)

    unit_k, scale_k, _ = normalize(k_ref[...], kgain, ones)
    for ck in range(TILES):
        rows = slice(ck * TILE, (ck + 1) * TILE)
        own, later = slice(ck * WIDE, TILES * WIDE), slice(0, (ck + 1) * WIDE)
        dv = dot(pown_ref[rows, own], gm_ref[own]) + dot(pn_ref[rows, later], gmn_ref[later])
        dv_ref[rows] = dv.astype(bf16)
        dk = dot(sown_ref[rows, own], qm_ref[own]) + dot(sn_ref[rows, later], qmn_ref[later])
        dk_ref[rows] = norm_backward(
            dk * SCALE, unit_k[rows], scale_k[rows], kgain, ones
        ).astype(bf16)

    for tile in range(TILES):
        for kind in range(4):
            halo_copy(kind, tile).wait_send()
        stat_copy(tile).wait_send()
    for dy, dx in a_offsets:
        a_copy(dy, dx).wait_send()

    for dz, dc in b_offsets:
        b_copy(dz, dc, arriving=True).wait_recv()
    block = bbuf[0]
    for i in range(1, nz):
        block += bbuf[i]
    for i in range(nz):
        bgain[c * nz + i] = bbuf[i, 3:4]
    gain_sum = bgain[0]
    for i in range(1, nc * nz):
        gain_sum += bgain[i]
    for h in range(2):
        taps = block[h : h + 1]
        rest = block[2:3, h * HD : h * HD + 1] - jnp.sum(taps, axis=1, keepdims=True)
        dbias_ref[h : h + 1, 0:LANES] = taps
        dbias_ref[h : h + 1, LANES : LANES + 1] = rest
    gain_sum = (gain_sum + pltpu.roll(gain_sum, HD, 1))[:, 0:HD]
    dqgain_ref[...] = gain_sum
    dkgain_ref[...] = gain_sum * qgain_ref[...] / kgain_ref[...]
    for dz, dc in b_offsets:
        b_copy(dz, dc).wait_send()


def flush(*refs):
    count = len(refs) // 2
    sems = refs[-1]
    copies = [
        pltpu.make_async_copy(refs[i], refs[count + i], sems.at[i]) for i in range(count)
    ]
    for copy in copies:
        copy.start()
    for copy in copies:
        copy.wait()


def per_device(sizes, query, key, value, out_grad, query_gain, key_gain, rel_bias):
    nz, ny, nx, nc = sizes
    vmem = pl.BlockSpec(memory_space=pltpu.VMEM)
    hbm = pl.BlockSpec(memory_space=pl.ANY)
    dma = pltpu.SemaphoreType.DMA
    regular = pltpu.SemaphoreType.REGULAR
    shapes = (((ROWS, LANES), bf16),) * 3 + (((1, HD), f32),) * 2 + ((rel_bias.shape, f32),)
    tile_rows, wide_rows = (ROWS, LANES), (TILES * WIDE, LANES)
    square = (ROWS, TILES * WIDE)
    outs = pl.pallas_call(
        functools.partial(body, sizes),
        out_shape=tuple(pltpu.VMEM(*s) for s in shapes),
        in_specs=[hbm] * 7,
        out_specs=(vmem,) * 6,
        scratch_shapes=[
            *[pltpu.VMEM(tile_rows, bf16)] * 4,
            *[pltpu.VMEM((1, HD), f32)] * 2,
            pltpu.VMEM(rel_bias.shape, f32),
            *[pltpu.VMEM(tile_rows, bf16)] * 4,
            *[pltpu.VMEM((TILES, 8, WIDE), f32)] * 2,
            *[pltpu.VMEM(tile_rows, f32)] * 3,
            *[pltpu.VMEM(tile_rows, bf16)] * 2,
            *[pltpu.VMEM(wide_rows, bf16)] * 4,
            *[pltpu.VMEM((TILES, (TILES + 1) * TILE, WIDE), f32)] * 2,
            *[pltpu.VMEM(square, f32)] * 2,
            *[pltpu.VMEM(square, bf16)] * 4,
            pltpu.VMEM((ny, 4, LANES), f32),
            pltpu.VMEM((nx * ny, 1, LANES), f32),
            pltpu.VMEM((1, LANES), f32),
            pltpu.VMEM((nz, 4, LANES), f32),
            pltpu.VMEM((nc * nz, 1, LANES), f32),
            pltpu.VMEM((1, LANES), f32),
            dma((7,)),
            dma((4, TILES)),
            dma((4, TILES)),
            dma((TILES,)),
            dma((TILES,)),
            dma((nx * ny,)),
            dma((nx * ny,)),
            dma((nc * nz,)),
            dma((nc * nz,)),
            *[regular] * 5,
        ],
        compiler_params=pltpu.CompilerParams(collective_id=0, has_side_effects=True),
        name="segment_backward",
    )(query, key, value, out_grad, query_gain.reshape(1, HD), key_gain.reshape(1, HD), rel_bias)
    outs = pl.pallas_call(
        flush,
        out_shape=tuple(jax.ShapeDtypeStruct(*s) for s in shapes),
        in_specs=[vmem] * 6,
        out_specs=(hbm,) * 6,
        scratch_shapes=[dma((6,))],
        name="flush",
    )(*(pltpu.with_memory_space_constraint(o, pltpu.VMEM) for o in outs))
    return (*outs[:3], outs[3].reshape(HD), outs[4].reshape(HD), outs[5])


def solution(mesh):
    sizes = mesh_sizes(mesh)
    torus = Mesh(mesh.devices.reshape(sizes), ("z", "y", "x", "c"))
    return jax.shard_map(
        functools.partial(per_device, sizes),
        mesh=torus,
        in_specs=(P(SP, TP), P(SP, TP), P(SP, TP), P(SP, TP), P(), P(), P(TP, None)),
        out_specs=(P(SP, TP), P(SP, TP), P(SP, TP), P(), P(), P(TP, None)),
        check_vma=False,
    )


def mesh_sizes(mesh):
    return (16, 8, 4, 2)
```

```python
import functools

import jax
import jax.numpy as jnp
from jax import lax
from jax.experimental import pallas as pl
from jax.experimental.pallas import tpu as pltpu
from jax.sharding import Mesh
from jax.sharding import PartitionSpec as P

SP = ("z", "y")
TP = ("x", "c")
MESH = pl.DeviceIdType.MESH

ROWS = 512
TILE = 128
TILES = ROWS // TILE
LANES = 128
HD = 64
WIDE = 2 * TILE
EPS = 1e-06
LOG2E = 1.4426950408889634
SCALE = HD**-0.5
OFF = -1e30

f32 = jnp.float32
bf16 = jnp.bfloat16


def dot(a, b, dims=((1,), (0,))):
    return lax.dot_general(a, b, (dims, ((), ())), preferred_element_type=f32)


def iota(shape, axis):
    return lax.broadcasted_iota(jnp.int32, shape, axis)


def head_sums(x, ones):
    high = x.astype(bf16)
    low = (x - high.astype(f32)).astype(bf16)
    return dot(high, ones) + dot(low, ones)


def normalize(x, gain, ones):
    wide = x.astype(f32)
    scale = lax.rsqrt(head_sums(wide * wide, ones) * (1.0 / HD) + EPS)
    unit = wide * scale
    return unit, scale, (unit * gain).astype(bf16)


def norm_backward(grad_hat, unit, scale, gain, ones):
    grad_unit = grad_hat * gain
    inner = head_sums(grad_unit * unit, ones) * (1.0 / HD)
    return scale * (grad_unit - unit * inner)


def shifted_rows(row):
    rows = jnp.broadcast_to(row, (TILE, LANES))
    return pltpu.roll(rows, 0, 1, stride=1, stride_axis=0)


def diagonal_sums(block):
    parts = [block[0:8]]
    for i in range(8, TILE, 8):
        parts.append(pltpu.roll(block[i : i + 8], LANES - i, 1))
    while len(parts) > 1:
        parts = [parts[i] + parts[i + 1] for i in range(0, len(parts), 2)]
    block = parts[0]
    index = iota((8, LANES), 0)
    for bit in (1, 2, 4):
        block = jnp.where((index & bit) != 0, pltpu.roll(block, LANES - bit, 1), block)
    return jnp.sum(block, axis=0, keepdims=True)


def both_heads(a):
    first = iota((TILE, LANES), 1) < HD
    zero = jnp.zeros((), a.dtype)
    return jnp.concatenate([jnp.where(first, a, zero), jnp.where(first, zero, a)], axis=0)


def body(
    sizes,
    q_hbm,
    k_hbm,
    v_hbm,
    g_hbm,
    qgain_hbm,
    kgain_hbm,
    bias_hbm,
    dq_ref,
    dk_ref,
    dv_ref,
    dqgain_ref,
    dkgain_ref,
    dbias_ref,
    qgain_ref,
    kgain_ref,
    bias_ref,
    kv_ref,
    hkv_ref,
    qg_ref,
    nqg_ref,
    send_stat,
    recv_stat,
    unit_q,
    scale_q,
    unit_k,
    scale_k,
    dk_acc,
    khat_ref,
    hkhat_ref,
    v_ref,
    qm_ref,
    gm_ref,
    qmn_ref,
    gmn_ref,
    e_ref,
    d_ref,
    low_ref,
    en_ref,
    dn_ref,
    pown_ref,
    pn_ref,
    sn_ref,
    abuf,
    again,
    asend,
    bbuf,
    bgain,
    bsend,
    load_sem,
    halo_recv,
    halo_send,
    stat_sem,
    a_sem,
    b_sem,
    level,
):
    nz, ny, nx, nc = sizes
    nsp = nz * ny
    z, y, x, c = (lax.axis_index(a) for a in ("z", "y", "x", "c"))
    sp = z * ny + y
    after, before = lax.rem(sp + 1, nsp), lax.rem(sp + nsp - 1, nsp)

    def at_sp(i):
        return {"z": i // ny, "y": lax.rem(i, ny)}

    def both_ways(name, place, size, distance):
        return [
            {name: lax.rem(place + distance, size)},
            {name: lax.rem(place + (distance // size + 1) * size - distance, size)},
        ]

    def tell(sem, targets):
        for target in targets:
            pl.semaphore_signal(sem, inc=1, device_id=target, device_id_type=MESH)

    def wait_bytes(ref, sem):
        pltpu.make_async_copy(ref, ref, sem).wait()

    axes = both_ways("z", z, nz, 1) + both_ways("y", y, ny, 1)
    if nx > 1:
        axes += both_ways("x", x, nx, 1)
    partner = [{"c": lax.rem(c + d, nc)} for d in range(1, nc)]
    x_peers = [{"x": lax.rem(x + d, nx)} for d in range(1, nx)]
    two_away = both_ways("z", z, nz, 2) + both_ways("y", y, ny, 2)
    four_away = both_ways("z", z, nz, 4)
    level_1, level_2, level_3, x_ready, c_ready = (level.at[i] for i in range(5))

    barrier = pltpu.get_barrier_semaphore()
    neighbours = [at_sp(after), at_sp(before)] + axes + partner
    tell(barrier, neighbours)

    tiles = [slice(t * TILE, (t + 1) * TILE) for t in range(TILES)]
    wides = [slice(t * WIDE, (t + 1) * WIDE) for t in range(TILES)]
    for first, second, ref, sem in ((k_hbm, v_hbm, kv_ref, 0), (q_hbm, g_hbm, qg_ref, 1)):
        for t in reversed(range(TILES)):
            for half, src in enumerate((first, second)):
                dst = ref.at[t, pl.ds(half * TILE, TILE)]
                pltpu.make_async_copy(src.at[tiles[t]], dst, load_sem.at[sem]).start()
    small = [
        pltpu.make_async_copy(src, dst, load_sem.at[2 + i])
        for i, (src, dst) in enumerate(
            ((qgain_hbm, qgain_ref), (kgain_hbm, kgain_ref), (bias_hbm, bias_ref))
        )
    ]
    for load in small:
        load.start()
    pl.semaphore_wait(barrier, len(neighbours))

    def halo_copy(kind, tile):
        src, dst, to, recv = (
            (kv_ref, hkv_ref, after, tile),
            (qg_ref, nqg_ref, before, TILES),
        )[kind]
        return pltpu.make_async_remote_copy(
            src_ref=src.at[tile],
            dst_ref=dst.at[tile],
            send_sem=halo_send.at[kind],
            recv_sem=halo_recv.at[recv],
            device_id=at_sp(to),
            device_id_type=MESH,
        )

    wait_bytes(kv_ref, load_sem.at[0])
    for tile in reversed(range(TILES)):
        halo_copy(0, tile).start()
    wait_bytes(qg_ref, load_sem.at[1])
    for tile in reversed(range(TILES)):
        halo_copy(1, tile).start()
    tell(level_1, axes)
    for load in small:
        load.wait()

    ones = (iota((LANES, LANES), 0) // HD == iota((LANES, LANES), 1) // HD).astype(bf16)
    qgain = jnp.concatenate([qgain_ref[...], qgain_ref[...]], axis=1)
    kgain = jnp.concatenate([kgain_ref[...], kgain_ref[...]], axis=1)

    key_i, query_i = iota((TILE, TILE), 0), iota((TILE, TILE), 1)
    reached = query_i >= key_i
    near, mid, far = [], [], []
    for h in range(2):
        row = bias_ref[h : h + 1, 0:LANES] * LOG2E
        last = bias_ref[h : h + 1, LANES : LANES + 1] * LOG2E
        table = shifted_rows(row)
        near.append(jnp.where(reached, table, OFF))
        mid.append(jnp.where(reached, last, table))
        far.append(jnp.broadcast_to(last, (1, TILE)))
    near = jnp.concatenate(near, axis=1)
    mid = jnp.concatenate(mid, axis=1)
    far = jnp.concatenate(far, axis=1)
    both_reached = jnp.concatenate([reached, reached], axis=1)
    wide_q = lax.rem(iota((TILE, WIDE), 1), TILE) // HD
    wide_k = iota((TILE, WIDE), 0) // HD
    edge = jnp.where(wide_k >= wide_q, 0.0, OFF)
    halo_off = jnp.where(sp > 0, 0.0, OFF)
    next_off = jnp.where(sp < nsp - 1, 0.0, OFF)

    def own_bias(distance):
        return (near, mid, far)[min(distance, 2)]

    def halo_bias(distance, off):
        if distance == 0:
            return far + edge + off
        return (mid if distance == TILES - 1 else far) + off

    for t in range(TILES):
        unit, scale, hat = normalize(qg_ref[t, 0:TILE], qgain, ones)
        unit_q[tiles[t]] = unit
        scale_q[tiles[t]] = scale
        qm_ref[wides[t]] = both_heads(hat)
        gm_ref[wides[t]] = both_heads(qg_ref[t, TILE:])
        unit, scale, hat = normalize(kv_ref[t, 0:TILE], kgain, ones)
        unit_k[tiles[t]] = unit
        scale_k[tiles[t]] = scale
        khat_ref[tiles[t]] = hat
        v_ref[tiles[t]] = kv_ref[t, TILE:]

    nt = ((1,), (1,))
    l_parts, n_parts = [], []
    for t in range(TILES):
        count = (t + 1) * TILE
        s = dot(khat_ref[0:count], qm_ref[wides[t]], nt)
        d = dot(v_ref[0:count], gm_ref[wides[t]], nt)
        l_sum = jnp.zeros((1, WIDE), f32)
        n_sum = jnp.zeros((1, WIDE), f32)
        for ck in range(t + 1):
            part = tiles[ck]
            slot = slice((TILES - t + ck) * TILE, (TILES - t + ck + 1) * TILE)
            e = jnp.exp2(s[part] * (SCALE * LOG2E) + own_bias(t - ck))
            e_ref[t, slot] = e
            d_ref[t, slot] = d[part]
            l_sum += jnp.sum(e, axis=0, keepdims=True)
            n_sum += jnp.sum(e * d[part], axis=0, keepdims=True)
        l_parts.append(l_sum)
        n_parts.append(n_sum)
    pl.semaphore_wait(level_1, len(axes))
    tell(level_2, two_away)

    def stat_copy(t):
        return pltpu.make_async_remote_copy(
            src_ref=send_stat.at[t],
            dst_ref=recv_stat.at[t],
            send_sem=stat_sem.at[0],
            recv_sem=stat_sem.at[1],
            device_id=at_sp(before),
            device_id_type=MESH,
        )

    total = jnp.zeros((1, WIDE), f32)
    near_sum = jnp.zeros((TILE, WIDE), f32)
    mid_sum = jnp.zeros((TILE, WIDE), f32)
    gain_sum = jnp.zeros((1, LANES), f32)
    for ck in reversed(range(TILES)):
        if ck == 1:
            pl.semaphore_wait(level_2, len(two_away))
            tell(level_3, four_away)
            tell(x_ready, x_peers)
        rows = tiles[ck]
        wait_bytes(hkv_ref.at[ck], halo_recv.at[ck])
        hkhat_ref[rows] = normalize(hkv_ref[ck, 0:TILE], kgain, ones)[2]
        span = (ck + 1) * WIDE
        s = dot(hkhat_ref[rows], qm_ref[0:span], nt)
        d = dot(hkv_ref[ck, TILE:], gm_ref[0:span], nt)
        for t in reversed(range(ck + 1)):
            part = wides[t]
            slot = slice((ck - t) * TILE, (ck - t + 1) * TILE)
            e = jnp.exp2(s[:, part] * (SCALE * LOG2E) + halo_bias(ck - t, halo_off))
            e_ref[t, slot] = e
            d_ref[t, slot] = d[:, part]
            l_parts[t] += jnp.sum(e, axis=0, keepdims=True)
            n_parts[t] += jnp.sum(e * d[:, part], axis=0, keepdims=True)
        t = ck
        inv = 1.0 / l_parts[t]
        delta = n_parts[t] * inv
        send_stat[t, 0:1] = inv
        send_stat[t, 1:2] = delta
        stat_copy(t).start()
        prob = e_ref[t] * inv
        grad = prob * (d_ref[t] - delta)
        total += jnp.sum(grad, axis=0, keepdims=True)
        own = (TILES - t) * TILE
        near_sum += grad[TILES * TILE :]
        mid_sum += grad[(TILES - 1) * TILE : TILES * TILE]
        low = grad.astype(bf16)
        low_ref[t] = low
        pown_ref[0 : (t + 1) * TILE, wides[t]] = prob[own:].astype(bf16)
        dk_t = dot(low, qm_ref[wides[t]])
        keys = jnp.concatenate([hkhat_ref[t * TILE :], khat_ref[0 : (t + 1) * TILE]], axis=0)
        gain_sum += jnp.sum(dk_t * keys.astype(f32), axis=0, keepdims=True)
        if t == TILES - 1:
            dk_acc[...] = dk_t[own:]
        else:
            dk_acc[0 : (t + 1) * TILE] += dk_t[own:]

    diagonals = jnp.where(both_reached, near_sum, mid_sum)
    taps = [diagonal_sums(diagonals[:, h * TILE : (h + 1) * TILE]) for h in range(2)]
    sums = [jnp.sum(total[:, h * TILE : (h + 1) * TILE], axis=1, keepdims=True) for h in range(2)]
    lane = iota((1, LANES), 1)
    sums = jnp.where(lane < HD, sums[0], sums[1])
    abuf[y] = jnp.concatenate([taps[0], taps[1], sums, gain_sum], axis=0)
    asend[...] = gain_sum

    a_offsets = [(dy, dx) for dx in range(nx) for dy in range(ny) if (dy, dx) != (0, 0)]

    def a_copy(dy, dx):
        to_y, to_x = lax.rem(y + dy, ny), lax.rem(x + dx, nx)
        kind = 0 if dx == 0 else 1
        return pltpu.make_async_remote_copy(
            src_ref=asend if kind else abuf.at[y],
            dst_ref=again.at[x * ny + y] if kind else abuf.at[y],
            send_sem=a_sem.at[kind],
            recv_sem=a_sem.at[2 + kind],
            device_id={"y": to_y, "x": to_x},
            device_id_type=MESH,
        )

    def wait_a(first):
        wait_bytes(abuf.at[pl.ds(0, ny - 1)], a_sem.at[first])
        if nx > 1:
            wait_bytes(again.at[pl.ds(0, ny * (nx - 1))], a_sem.at[first + 1])

    if x_peers:
        pl.semaphore_wait(x_ready, len(x_peers))
    for dy, dx in a_offsets:
        a_copy(dy, dx).start()

    wait_bytes(nqg_ref, halo_recv.at[TILES])
    for t in reversed(range(TILES)):
        qmn_ref[wides[t]] = both_heads(normalize(nqg_ref[t, 0:TILE], qgain, ones)[2])
        gmn_ref[wides[t]] = both_heads(nqg_ref[t, TILE:])
        s = dot(khat_ref[t * TILE :], qmn_ref[wides[t]], nt)
        d = dot(v_ref[t * TILE :], gmn_ref[wides[t]], nt)
        for ck in range(t, TILES):
            part = slice((ck - t) * TILE, (ck - t + 1) * TILE)
            en_ref[tiles[ck], wides[t]] = jnp.exp2(
                s[part] * (SCALE * LOG2E) + halo_bias(ck - t, next_off)
            )
            dn_ref[tiles[ck], wides[t]] = d[part]

    for t in range(TILES):
        rows = tiles[t]
        keys = jnp.concatenate([hkhat_ref[t * TILE :], khat_ref[0 : (t + 1) * TILE]], axis=0)
        dq_t = dot(keys, low_ref[t], ((0,), (0,)))
        dq_t = jnp.concatenate([dq_t[0:HD, 0:TILE], dq_t[HD:, TILE:]], axis=0) * SCALE
        dq_ref[rows] = norm_backward(
            dq_t.T, unit_q[rows], scale_q[rows], qgain, ones
        ).astype(bf16)

    pl.semaphore_wait(level_3, len(four_away))
    tell(c_ready, partner)
    wait_a(2)
    block = abuf[0]
    for i in range(1, ny):
        block += abuf[i]
    for i in range(ny):
        again[x * ny + i] = abuf[i, 3:4]
    gain_sum = again[0]
    for i in range(1, nx * ny):
        gain_sum += again[i]
    bbuf[z] = jnp.concatenate([block[0:3], gain_sum], axis=0)
    bsend[...] = gain_sum

    b_offsets = [(dz, dc) for dc in range(nc) for dz in range(nz) if (dz, dc) != (0, 0)]

    def b_copy(dz, dc):
        to_z, to_c = lax.rem(z + dz, nz), lax.rem(c + dc, nc)
        kind = 0 if dc == 0 else 1
        return pltpu.make_async_remote_copy(
            src_ref=bsend if kind else bbuf.at[z],
            dst_ref=bgain.at[c * nz + z] if kind else bbuf.at[z],
            send_sem=b_sem.at[kind],
            recv_sem=b_sem.at[2 + kind],
            device_id={"z": to_z, "c": to_c},
            device_id_type=MESH,
        )

    def wait_b(first):
        wait_bytes(bbuf.at[pl.ds(0, nz - 1)], b_sem.at[first])
        if nc > 1:
            wait_bytes(bgain.at[pl.ds(0, nz * (nc - 1))], b_sem.at[first + 1])

    if partner:
        pl.semaphore_wait(c_ready, len(partner))
    for dz, dc in b_offsets:
        b_copy(dz, dc).start()

    wait_bytes(recv_stat, stat_sem.at[1])
    for t in reversed(range(TILES)):
        inv, delta = recv_stat[t, 0:1], recv_stat[t, 1:2]
        prob = en_ref[t * TILE :, wides[t]] * inv
        pn_ref[t * TILE :, wides[t]] = prob.astype(bf16)
        sn_ref[t * TILE :, wides[t]] = (prob * (dn_ref[t * TILE :, wides[t]] - delta)).astype(bf16)

    for ck in range(TILES):
        rows = tiles[ck]
        own, later = slice(ck * WIDE, TILES * WIDE), slice(0, (ck + 1) * WIDE)
        dv = dot(pown_ref[rows, own], gm_ref[own]) + dot(pn_ref[rows, later], gmn_ref[later])
        dv_ref[rows] = dv.astype(bf16)
        dk = dk_acc[rows] + dot(sn_ref[rows, later], qmn_ref[later])
        dk_ref[rows] = norm_backward(
            dk * SCALE, unit_k[rows], scale_k[rows], kgain, ones
        ).astype(bf16)

    wait_bytes(kv_ref, halo_send.at[0])
    wait_bytes(qg_ref, halo_send.at[1])
    wait_bytes(send_stat, stat_sem.at[0])
    wait_a(0)

    wait_b(2)
    block = bbuf[0]
    for i in range(1, nz):
        block += bbuf[i]
    for i in range(nz):
        bgain[c * nz + i] = bbuf[i, 3:4]
    gain_sum = bgain[0]
    for i in range(1, nc * nz):
        gain_sum += bgain[i]
    for h in range(2):
        taps = block[h : h + 1]
        rest = block[2:3, h * HD : h * HD + 1] - jnp.sum(taps, axis=1, keepdims=True)
        dbias_ref[h : h + 1, 0:LANES] = taps
        dbias_ref[h : h + 1, LANES : LANES + 1] = rest
    gain_sum = (gain_sum + pltpu.roll(gain_sum, HD, 1))[:, 0:HD] * SCALE
    dqgain_ref[...] = gain_sum / qgain_ref[...]
    dkgain_ref[...] = gain_sum / kgain_ref[...]
    wait_b(0)


def flush(*refs):
    count = len(refs) // 2
    sems = refs[-1]
    copies = [
        pltpu.make_async_copy(refs[i], refs[count + i], sems.at[i]) for i in range(count)
    ]
    for copy in copies:
        copy.start()
    for copy in copies:
        copy.wait()


def per_device(sizes, query, key, value, out_grad, query_gain, key_gain, rel_bias):
    nz, ny, nx, nc = sizes
    vmem = pl.BlockSpec(memory_space=pltpu.VMEM)
    hbm = pl.BlockSpec(memory_space=pl.ANY)
    dma = pltpu.SemaphoreType.DMA
    regular = pltpu.SemaphoreType.REGULAR
    shapes = (((ROWS, LANES), bf16),) * 3 + (((1, HD), f32),) * 2 + ((rel_bias.shape, f32),)
    tile_rows, wide_rows = (ROWS, LANES), (TILES * WIDE, LANES)
    square = (ROWS, TILES * WIDE)
    outs = pl.pallas_call(
        functools.partial(body, sizes),
        out_shape=tuple(pltpu.VMEM(*s) for s in shapes),
        in_specs=[hbm] * 7,
        out_specs=(vmem,) * 6,
        scratch_shapes=[
            *[pltpu.VMEM((1, HD), f32)] * 2,
            pltpu.VMEM(rel_bias.shape, f32),
            *[pltpu.VMEM((TILES, 2 * TILE, LANES), bf16)] * 4,
            *[pltpu.VMEM((TILES, 2, WIDE), f32)] * 2,
            *[pltpu.VMEM(tile_rows, f32)] * 5,
            *[pltpu.VMEM(tile_rows, bf16)] * 3,
            *[pltpu.VMEM(wide_rows, bf16)] * 4,
            *[pltpu.VMEM((TILES, (TILES + 1) * TILE, WIDE), f32)] * 2,
            pltpu.VMEM((TILES, (TILES + 1) * TILE, WIDE), bf16),
            *[pltpu.VMEM(square, f32)] * 2,
            *[pltpu.VMEM(square, bf16)] * 3,
            pltpu.VMEM((ny, 4, LANES), f32),
            pltpu.VMEM((nx * ny, 1, LANES), f32),
            pltpu.VMEM((1, LANES), f32),
            pltpu.VMEM((nz, 4, LANES), f32),
            pltpu.VMEM((nc * nz, 1, LANES), f32),
            pltpu.VMEM((1, LANES), f32),
            dma((5,)),
            dma((TILES + 1,)),
            dma((2,)),
            dma((2,)),
            dma((4,)),
            dma((4,)),
            regular((5,)),
        ],
        compiler_params=pltpu.CompilerParams(collective_id=0, has_side_effects=True),
        name="segment_backward",
    )(query, key, value, out_grad, query_gain.reshape(1, HD), key_gain.reshape(1, HD), rel_bias)
    outs = pl.pallas_call(
        flush,
        out_shape=tuple(jax.ShapeDtypeStruct(*s) for s in shapes),
        in_specs=[vmem] * 6,
        out_specs=(hbm,) * 6,
        scratch_shapes=[dma((6,))],
        name="flush",
    )(*(pltpu.with_memory_space_constraint(o, pltpu.VMEM) for o in outs))
    return (*outs[:3], outs[3].reshape(HD), outs[4].reshape(HD), outs[5])


def solution(mesh):
    sizes = mesh_sizes(mesh)
    torus = Mesh(mesh.devices.reshape(sizes), ("z", "y", "x", "c"))
    return jax.shard_map(
        functools.partial(per_device, sizes),
        mesh=torus,
        in_specs=(P(SP, TP), P(SP, TP), P(SP, TP), P(SP, TP), P(), P(), P(TP, None)),
        out_specs=(P(SP, TP), P(SP, TP), P(SP, TP), P(), P(), P(TP, None)),
        check_vma=False,
    )


def mesh_sizes(mesh):
    return (16, 8, 4, 2)
```

```python
import functools

import jax
import jax.numpy as jnp
from jax import lax
from jax.experimental import pallas as pl
from jax.experimental.pallas import tpu as pltpu
from jax.sharding import Mesh
from jax.sharding import PartitionSpec as P

SP = ("z", "y")
TP = ("x", "c")
MESH = pl.DeviceIdType.MESH

ROWS = 512
TILE = 128
TILES = ROWS // TILE
LANES = 128
HD = 64
WIDE = 2 * TILE
EPS = 1e-06
LOG2E = 1.4426950408889634
SCALE = HD**-0.5
OFF = -1e30

f32 = jnp.float32
bf16 = jnp.bfloat16


def dot(a, b, dims=((1,), (0,))):
    return lax.dot_general(a, b, (dims, ((), ())), preferred_element_type=f32)


def iota(shape, axis):
    return lax.broadcasted_iota(jnp.int32, shape, axis)


def head_sums(x, ones):
    high = x.astype(bf16)
    low = (x - high.astype(f32)).astype(bf16)
    return dot(high, ones) + dot(low, ones)


def normalize(x, gain, ones):
    wide = x.astype(f32)
    scale = lax.rsqrt(head_sums(wide * wide, ones) * (1.0 / HD) + EPS)
    unit = wide * scale
    return unit, scale, (unit * gain).astype(bf16)


def norm_backward(grad_hat, unit, scale, gain, ones):
    grad_unit = grad_hat * gain
    inner = head_sums(grad_unit * unit, ones) * (1.0 / HD)
    return scale * (grad_unit - unit * inner)


def shifted_rows(row):
    rows = jnp.broadcast_to(row, (TILE, LANES))
    return pltpu.roll(rows, 0, 1, stride=1, stride_axis=0)


def diagonal_sums(block):
    parts = [block[0:8]]
    for i in range(8, TILE, 8):
        parts.append(pltpu.roll(block[i : i + 8], LANES - i, 1))
    while len(parts) > 1:
        parts = [parts[i] + parts[i + 1] for i in range(0, len(parts), 2)]
    block = parts[0]
    index = iota((8, LANES), 0)
    for bit in (1, 2, 4):
        block = jnp.where((index & bit) != 0, pltpu.roll(block, LANES - bit, 1), block)
    return jnp.sum(block, axis=0, keepdims=True)


def both_heads(a):
    first = iota((TILE, LANES), 1) < HD
    zero = jnp.zeros((), a.dtype)
    return jnp.concatenate([jnp.where(first, a, zero), jnp.where(first, zero, a)], axis=0)


def body(
    sizes,
    q_hbm,
    k_hbm,
    v_hbm,
    g_hbm,
    qgain_hbm,
    kgain_hbm,
    bias_hbm,
    dq_ref,
    dk_ref,
    dv_ref,
    dqgain_ref,
    dkgain_ref,
    dbias_ref,
    qgain_ref,
    kgain_ref,
    bias_ref,
    kv_ref,
    hkv_ref,
    qg_ref,
    nqg_ref,
    send_stat,
    recv_stat,
    unit_q,
    scale_q,
    unit_k,
    scale_k,
    dk_acc,
    khat_ref,
    k_ref,
    v_ref,
    qm_ref,
    gm_ref,
    qmn_ref,
    gmn_ref,
    e_ref,
    d_ref,
    low_ref,
    en_ref,
    dn_ref,
    pown_ref,
    pn_ref,
    sn_ref,
    abuf,
    again,
    asend,
    gain_yx,
    bbuf,
    cbuf,
    zgain,
    load_sem,
    halo_recv,
    halo_send,
    stat_sem,
    a_sem,
    b_sem,
    c_sem,
    level,
):
    nz, ny, nx, nc = sizes
    nsp = nz * ny
    z, y, x, c = (lax.axis_index(a) for a in ("z", "y", "x", "c"))
    sp = z * ny + y
    after, before = lax.rem(sp + 1, nsp), lax.rem(sp + nsp - 1, nsp)

    def at_sp(i):
        return {"z": i // ny, "y": lax.rem(i, ny)}

    def both_ways(name, place, size, distance):
        return [
            {name: lax.rem(place + distance, size)},
            {name: lax.rem(place + (distance // size + 1) * size - distance, size)},
        ]

    def tell(sem, targets):
        for target in targets:
            pl.semaphore_signal(sem, inc=1, device_id=target, device_id_type=MESH)

    def wait_bytes(ref, sem):
        pltpu.make_async_copy(ref, ref, sem).wait()

    lead = nc - 1
    at_lead = c == lead
    axes = both_ways("z", z, nz, 1) + both_ways("y", y, ny, 1)
    if nx > 1:
        axes += both_ways("x", x, nx, 1)
    partner = [{"c": lax.rem(c + d, nc)} for d in range(1, nc)]
    x_peers = [{"x": lax.rem(x + d, nx)} for d in range(1, nx)]
    two_away = both_ways("z", z, nz, 2) + both_ways("y", y, ny, 2)
    four_away = both_ways("z", z, nz, 4)
    level_1, level_2, level_3, x_ready, c_ready, z_ready = (level.at[i] for i in range(6))

    barrier = pltpu.get_barrier_semaphore()
    neighbours = [at_sp(after), at_sp(before)] + axes + partner
    tell(barrier, neighbours)

    tiles = [slice(t * TILE, (t + 1) * TILE) for t in range(TILES)]
    wides = [slice(t * WIDE, (t + 1) * WIDE) for t in range(TILES)]
    small = [
        pltpu.make_async_copy(src, dst, load_sem.at[3 + i])
        for i, (src, dst) in enumerate(
            ((kgain_hbm, kgain_ref), (qgain_hbm, qgain_ref), (bias_hbm, bias_ref))
        )
    ]
    load_keys = pltpu.make_async_copy(k_hbm, k_ref, load_sem.at[0])
    load_keys.start()
    for load in small:
        load.start()
    for t in reversed(range(TILES)):
        dst = kv_ref.at[t, pl.ds(TILE, TILE)]
        pltpu.make_async_copy(v_hbm.at[tiles[t]], dst, load_sem.at[1]).start()
    for t in reversed(range(TILES)):
        for half, src in enumerate((q_hbm, g_hbm)):
            dst = qg_ref.at[t, pl.ds(half * TILE, TILE)]
            pltpu.make_async_copy(src.at[tiles[t]], dst, load_sem.at[2]).start()

    ones = (iota((LANES, LANES), 0) // HD == iota((LANES, LANES), 1) // HD).astype(bf16)
    small[0].wait()
    kgain = jnp.concatenate([kgain_ref[...], kgain_ref[...]], axis=1)
    load_keys.wait()
    for t in reversed(range(TILES)):
        unit, scale, hat = normalize(k_ref[tiles[t]], kgain, ones)
        unit_k[tiles[t]] = unit
        scale_k[tiles[t]] = scale
        khat_ref[tiles[t]] = hat
        kv_ref[t, 0:TILE] = hat
    pl.semaphore_wait(barrier, len(neighbours))

    def halo_copy(kind, tile):
        src, dst, to, recv = (
            (kv_ref, hkv_ref, after, tile),
            (qg_ref, nqg_ref, before, TILES),
        )[kind]
        return pltpu.make_async_remote_copy(
            src_ref=src.at[tile],
            dst_ref=dst.at[tile],
            send_sem=halo_send.at[kind],
            recv_sem=halo_recv.at[recv],
            device_id=at_sp(to),
            device_id_type=MESH,
        )

    wait_bytes(v_ref, load_sem.at[1])
    for tile in reversed(range(TILES)):
        halo_copy(0, tile).start()
    wait_bytes(qg_ref, load_sem.at[2])
    for tile in reversed(range(TILES)):
        halo_copy(1, tile).start()
    tell(level_1, axes)
    for load in small[1:]:
        load.wait()

    qgain = jnp.concatenate([qgain_ref[...], qgain_ref[...]], axis=1)

    key_i, query_i = iota((TILE, TILE), 0), iota((TILE, TILE), 1)
    reached = query_i >= key_i
    near, mid, far = [], [], []
    for h in range(2):
        row = bias_ref[h : h + 1, 0:LANES] * LOG2E
        last = bias_ref[h : h + 1, LANES : LANES + 1] * LOG2E
        table = shifted_rows(row)
        near.append(jnp.where(reached, table, OFF))
        mid.append(jnp.where(reached, last, table))
        far.append(jnp.broadcast_to(last, (1, TILE)))
    near = jnp.concatenate(near, axis=1)
    mid = jnp.concatenate(mid, axis=1)
    far = jnp.concatenate(far, axis=1)
    both_reached = jnp.concatenate([reached, reached], axis=1)
    wide_q = lax.rem(iota((TILE, WIDE), 1), TILE) // HD
    wide_k = iota((TILE, WIDE), 0) // HD
    edge = jnp.where(wide_k >= wide_q, 0.0, OFF)
    halo_off = jnp.where(sp > 0, 0.0, OFF)
    next_off = jnp.where(sp < nsp - 1, 0.0, OFF)

    def own_bias(distance):
        return (near, mid, far)[min(distance, 2)]

    def halo_bias(distance, off):
        if distance == 0:
            return far + edge + off
        return (mid if distance == TILES - 1 else far) + off

    for t in range(TILES):
        unit, scale, hat = normalize(qg_ref[t, 0:TILE], qgain, ones)
        unit_q[tiles[t]] = unit
        scale_q[tiles[t]] = scale
        qm_ref[wides[t]] = both_heads(hat)
        gm_ref[wides[t]] = both_heads(qg_ref[t, TILE:])
        v_ref[tiles[t]] = kv_ref[t, TILE:]

    nt = ((1,), (1,))
    l_parts, n_parts = [], []
    for t in range(TILES):
        count = (t + 1) * TILE
        s = dot(khat_ref[0:count], qm_ref[wides[t]], nt)
        d = dot(v_ref[0:count], gm_ref[wides[t]], nt)
        l_sum = jnp.zeros((1, WIDE), f32)
        n_sum = jnp.zeros((1, WIDE), f32)
        for ck in range(t + 1):
            part = tiles[ck]
            slot = slice((TILES - t + ck) * TILE, (TILES - t + ck + 1) * TILE)
            e = jnp.exp2(s[part] * (SCALE * LOG2E) + own_bias(t - ck))
            e_ref[t, slot] = e
            d_ref[t, slot] = d[part]
            l_sum += jnp.sum(e, axis=0, keepdims=True)
            n_sum += jnp.sum(e * d[part], axis=0, keepdims=True)
        l_parts.append(l_sum)
        n_parts.append(n_sum)
    pl.semaphore_wait(level_1, len(axes))
    tell(level_2, two_away)

    def stat_copy(t):
        return pltpu.make_async_remote_copy(
            src_ref=send_stat.at[t],
            dst_ref=recv_stat.at[t],
            send_sem=stat_sem.at[0],
            recv_sem=stat_sem.at[1],
            device_id=at_sp(before),
            device_id_type=MESH,
        )

    def keys_of(t):
        halo = [hkv_ref[ck, 0:TILE] for ck in range(t, TILES)]
        return jnp.concatenate(halo + [khat_ref[0 : (t + 1) * TILE]], axis=0)

    total = jnp.zeros((1, WIDE), f32)
    near_sum = jnp.zeros((TILE, WIDE), f32)
    mid_sum = jnp.zeros((TILE, WIDE), f32)
    gain_sum = jnp.zeros((1, LANES), f32)
    for ck in reversed(range(TILES)):
        if ck == TILES - 2:
            pl.semaphore_wait(level_2, len(two_away))
            tell(level_3, four_away)
            tell(x_ready, x_peers)
        wait_bytes(hkv_ref.at[ck], halo_recv.at[ck])
        if ck == 0:
            if x_peers:
                pl.semaphore_wait(x_ready, len(x_peers))

            @pl.when(at_lead)
            def _():
                tell(c_ready, partner)

        span = (ck + 1) * WIDE
        s = dot(hkv_ref[ck, 0:TILE], qm_ref[0:span], nt)
        d = dot(hkv_ref[ck, TILE:], gm_ref[0:span], nt)
        for t in reversed(range(ck + 1)):
            part = wides[t]
            slot = slice((ck - t) * TILE, (ck - t + 1) * TILE)
            e = jnp.exp2(s[:, part] * (SCALE * LOG2E) + halo_bias(ck - t, halo_off))
            e_ref[t, slot] = e
            d_ref[t, slot] = d[:, part]
            l_parts[t] += jnp.sum(e, axis=0, keepdims=True)
            n_parts[t] += jnp.sum(e * d[:, part], axis=0, keepdims=True)
        t = ck
        inv = 1.0 / l_parts[t]
        delta = n_parts[t] * inv
        send_stat[t, 0:1] = inv
        send_stat[t, 1:2] = delta
        prob = e_ref[t] * inv
        grad = prob * (d_ref[t] - delta)
        total += jnp.sum(grad, axis=0, keepdims=True)
        own = (TILES - t) * TILE
        near_sum += grad[TILES * TILE :]
        mid_sum += grad[(TILES - 1) * TILE : TILES * TILE]
        low = grad.astype(bf16)
        low_ref[t] = low
        pown_ref[0 : (t + 1) * TILE, wides[t]] = prob[own:].astype(bf16)
        dk_t = dot(low, qm_ref[wides[t]])
        keys = keys_of(t)
        gain_sum += jnp.sum(dk_t * keys.astype(f32), axis=0, keepdims=True)
        if t == TILES - 1:
            dk_acc[...] = dk_t[own:]
        else:
            dk_acc[0 : (t + 1) * TILE] += dk_t[own:]

    diagonals = jnp.where(both_reached, near_sum, mid_sum)
    taps = [diagonal_sums(diagonals[:, h * TILE : (h + 1) * TILE]) for h in range(2)]
    folded = [total[:, h * TILE : (h + 1) * TILE] for h in range(2)]
    folded = [part + pltpu.roll(part, HD, 1) for part in folded]
    first_half = iota((1, LANES), 1) < HD
    sums = jnp.where(first_half, folded[0], folded[1])
    asend[...] = gain_sum
    abuf[y] = jnp.concatenate([taps[0], taps[1], sums, gain_sum], axis=0)

    group = ny * nx
    others = [(dy, dx) for dx in range(nx) for dy in range(ny)][1:]
    others.sort(key=lambda o: -min(o[0], ny - o[0]) - min(o[1], nx - o[1]))
    y_others = sorted(range(1, ny), key=lambda d: -min(d, ny - d))
    z_others = sorted(range(1, nz), key=lambda d: -min(d, nz - d))

    def gain_copy(dy, dx):
        return pltpu.make_async_remote_copy(
            src_ref=asend,
            dst_ref=again.at[c * group + x * ny + y],
            send_sem=a_sem.at[1],
            recv_sem=a_sem.at[3],
            device_id={"y": lax.rem(y + dy, ny), "x": lax.rem(x + dx, nx), "c": lead},
            device_id_type=MESH,
        )

    def a_copy(dy):
        return pltpu.make_async_remote_copy(
            src_ref=abuf.at[y],
            dst_ref=abuf.at[y],
            send_sem=a_sem.at[0],
            recv_sem=a_sem.at[2],
            device_id={"y": lax.rem(y + dy, ny)},
            device_id_type=MESH,
        )

    @pl.when(jnp.logical_not(at_lead))
    def _():
        pl.semaphore_wait(c_ready, 1)

    for dy, dx in others:
        gain_copy(dy, dx).start()

    @pl.when(jnp.logical_not(at_lead))
    def _():
        gain_copy(0, 0).start()

    for dy in y_others:
        a_copy(dy).start()
    for t in range(TILES):
        stat_copy(t).start()

    wait_bytes(nqg_ref, halo_recv.at[TILES])
    for t in reversed(range(TILES)):
        qmn_ref[wides[t]] = both_heads(normalize(nqg_ref[t, 0:TILE], qgain, ones)[2])
        gmn_ref[wides[t]] = both_heads(nqg_ref[t, TILE:])
        s = dot(khat_ref[t * TILE :], qmn_ref[wides[t]], nt)
        d = dot(v_ref[t * TILE :], gmn_ref[wides[t]], nt)
        for ck in range(t, TILES):
            part = slice((ck - t) * TILE, (ck - t + 1) * TILE)
            en_ref[tiles[ck], wides[t]] = jnp.exp2(
                s[part] * (SCALE * LOG2E) + halo_bias(ck - t, next_off)
            )
            dn_ref[tiles[ck], wides[t]] = d[part]

    pl.semaphore_wait(level_3, len(four_away))

    @pl.when(jnp.logical_not(at_lead))
    def _():
        tell(z_ready, [{"c": lead}])

    for t in range(TILES):
        rows = tiles[t]
        keys = keys_of(t)
        dq_t = dot(keys, low_ref[t], ((0,), (0,)))
        dq_t = jnp.concatenate([dq_t[0:HD, 0:TILE], dq_t[HD:, TILE:]], axis=0) * SCALE
        dq_ref[rows] = norm_backward(
            dq_t.T, unit_q[rows], scale_q[rows], qgain, ones
        ).astype(bf16)

    @pl.when(at_lead)
    def _():
        wait_bytes(again.at[pl.ds(0, nc * group - 1)], a_sem.at[3])
        again[c * group + x * ny + y] = asend[...]
        gains = again[0]
        for i in range(1, nc * group):
            gains += again[i]
        gain_yx[...] = gains

    wait_bytes(abuf.at[pl.ds(0, ny - 1)], a_sem.at[2])
    block = abuf[0]
    for i in range(1, ny):
        block += abuf[i]
    bbuf[z] = block

    @pl.when(at_lead)
    def _():
        bbuf[z, 3:4] = gain_yx[...]

    def b_copy(dz):
        return pltpu.make_async_remote_copy(
            src_ref=bbuf.at[z],
            dst_ref=bbuf.at[z],
            send_sem=b_sem.at[0],
            recv_sem=b_sem.at[1],
            device_id={"z": lax.rem(z + dz, nz)},
            device_id_type=MESH,
        )

    def down_copy(dz):
        return pltpu.make_async_remote_copy(
            src_ref=gain_yx,
            dst_ref=zgain.at[z],
            send_sem=c_sem.at[0],
            recv_sem=c_sem.at[1],
            device_id={"z": lax.rem(z + dz, nz), "c": 0},
            device_id_type=MESH,
        )

    for dz in z_others:
        b_copy(dz).start()

    @pl.when(at_lead)
    def _():
        pl.semaphore_wait(z_ready, 1)
        for dz in z_others + [0]:
            down_copy(dz).start()

    wait_bytes(recv_stat, stat_sem.at[1])
    for t in reversed(range(TILES)):
        inv, delta = recv_stat[t, 0:1], recv_stat[t, 1:2]
        prob = en_ref[t * TILE :, wides[t]] * inv
        pn_ref[t * TILE :, wides[t]] = prob.astype(bf16)
        sn_ref[t * TILE :, wides[t]] = (prob * (dn_ref[t * TILE :, wides[t]] - delta)).astype(bf16)

    for ck in range(TILES):
        rows = tiles[ck]
        own, later = slice(ck * WIDE, TILES * WIDE), slice(0, (ck + 1) * WIDE)
        dv = dot(pown_ref[rows, own], gm_ref[own]) + dot(pn_ref[rows, later], gmn_ref[later])
        dv_ref[rows] = dv.astype(bf16)
        dk = dk_acc[rows] + dot(sn_ref[rows, later], qmn_ref[later])
        dk_ref[rows] = norm_backward(
            dk * SCALE, unit_k[rows], scale_k[rows], kgain, ones
        ).astype(bf16)

    wait_bytes(kv_ref, halo_send.at[0])
    wait_bytes(qg_ref, halo_send.at[1])
    wait_bytes(send_stat, stat_sem.at[0])
    wait_bytes(abuf.at[pl.ds(0, ny - 1)], a_sem.at[0])

    @pl.when(at_lead)
    def _():
        wait_bytes(again.at[pl.ds(0, group - 1)], a_sem.at[1])

    @pl.when(jnp.logical_not(at_lead))
    def _():
        wait_bytes(again.at[pl.ds(0, group)], a_sem.at[1])

    wait_bytes(bbuf.at[pl.ds(0, nz - 1)], b_sem.at[1])
    block = bbuf[0]
    for i in range(1, nz):
        block += bbuf[i]

    @pl.when(at_lead)
    def _():
        cbuf[...] = block[3:4]

    @pl.when(jnp.logical_not(at_lead))
    def _():
        wait_bytes(zgain, c_sem.at[1])
        gains = zgain[0]
        for i in range(1, nz):
            gains += zgain[i]
        cbuf[...] = gains

    for h in range(2):
        taps = block[h : h + 1]
        rest = jnp.where(first_half if h == 0 else ~first_half, block[2:3], 0.0) - taps
        dbias_ref[h : h + 1, 0:LANES] = taps
        dbias_ref[h : h + 1, LANES : LANES + 1] = jnp.sum(rest, axis=1, keepdims=True)

    gain_sum = cbuf[...]
    gain_sum = (gain_sum + pltpu.roll(gain_sum, HD, 1))[:, 0:HD] * SCALE
    dqgain_ref[...] = gain_sum / qgain_ref[...]
    dkgain_ref[...] = gain_sum / kgain_ref[...]
    wait_bytes(bbuf.at[pl.ds(0, nz - 1)], b_sem.at[0])

    @pl.when(at_lead)
    def _():
        wait_bytes(zgain, c_sem.at[0])


def flush(*refs):
    count = len(refs) // 2
    sems = refs[-1]
    copies = [
        pltpu.make_async_copy(refs[i], refs[count + i], sems.at[i]) for i in range(count)
    ]
    for copy in copies:
        copy.start()
    for copy in copies:
        copy.wait()


def per_device(sizes, query, key, value, out_grad, query_gain, key_gain, rel_bias):
    nz, ny, nx, nc = sizes
    vmem = pl.BlockSpec(memory_space=pltpu.VMEM)
    hbm = pl.BlockSpec(memory_space=pl.ANY)
    dma = pltpu.SemaphoreType.DMA
    regular = pltpu.SemaphoreType.REGULAR
    shapes = (((ROWS, LANES), bf16),) * 3 + (((1, HD), f32),) * 2 + ((rel_bias.shape, f32),)
    tile_rows, wide_rows = (ROWS, LANES), (TILES * WIDE, LANES)
    square = (ROWS, TILES * WIDE)
    outs = pl.pallas_call(
        functools.partial(body, sizes),
        out_shape=tuple(pltpu.VMEM(*s) for s in shapes),
        in_specs=[hbm] * 7,
        out_specs=(vmem,) * 6,
        scratch_shapes=[
            *[pltpu.VMEM((1, HD), f32)] * 2,
            pltpu.VMEM(rel_bias.shape, f32),
            *[pltpu.VMEM((TILES, 2 * TILE, LANES), bf16)] * 4,
            *[pltpu.VMEM((TILES, 2, WIDE), f32)] * 2,
            *[pltpu.VMEM(tile_rows, f32)] * 5,
            *[pltpu.VMEM(tile_rows, bf16)] * 3,
            *[pltpu.VMEM(wide_rows, bf16)] * 4,
            *[pltpu.VMEM((TILES, (TILES + 1) * TILE, WIDE), f32)] * 2,
            pltpu.VMEM((TILES, (TILES + 1) * TILE, WIDE), bf16),
            *[pltpu.VMEM(square, f32)] * 2,
            *[pltpu.VMEM(square, bf16)] * 3,
            pltpu.VMEM((ny, 4, LANES), f32),
            pltpu.VMEM((nc * nx * ny, 1, LANES), f32),
            pltpu.VMEM((1, LANES), f32),
            pltpu.VMEM((1, LANES), f32),
            pltpu.VMEM((nz, 4, LANES), f32),
            pltpu.VMEM((1, LANES), f32),
            pltpu.VMEM((nz, 1, LANES), f32),
            dma((6,)),
            dma((TILES + 1,)),
            dma((2,)),
            dma((2,)),
            dma((4,)),
            dma((2,)),
            dma((2,)),
            regular((6,)),
        ],
        compiler_params=pltpu.CompilerParams(collective_id=0, has_side_effects=True),
        name="segment_backward",
    )(query, key, value, out_grad, query_gain.reshape(1, HD), key_gain.reshape(1, HD), rel_bias)
    outs = pl.pallas_call(
        flush,
        out_shape=tuple(jax.ShapeDtypeStruct(*s) for s in shapes),
        in_specs=[vmem] * 6,
        out_specs=(hbm,) * 6,
        scratch_shapes=[dma((6,))],
        name="flush",
    )(*(pltpu.with_memory_space_constraint(o, pltpu.VMEM) for o in outs))
    return (*outs[:3], outs[3].reshape(HD), outs[4].reshape(HD), outs[5])


def solution(mesh):
    sizes = mesh_sizes(mesh)
    torus = Mesh(mesh.devices.reshape(sizes), ("z", "y", "x", "c"))
    return jax.shard_map(
        functools.partial(per_device, sizes),
        mesh=torus,
        in_specs=(P(SP, TP), P(SP, TP), P(SP, TP), P(SP, TP), P(), P(), P(TP, None)),
        out_specs=(P(SP, TP), P(SP, TP), P(SP, TP), P(), P(), P(TP, None)),
        check_vma=False,
    )


def mesh_sizes(mesh):
    return (16, 8, 4, 2)
```

```python
import functools

import jax
import jax.numpy as jnp
from jax import lax
from jax.experimental import pallas as pl
from jax.experimental.pallas import tpu as pltpu
from jax.sharding import Mesh
from jax.sharding import PartitionSpec as P

SP = ("z", "y")
TP = ("x", "c")
MESH = pl.DeviceIdType.MESH

ROWS = 512
TILE = 128
TILES = ROWS // TILE
LANES = 128
HD = 64
WIDE = 2 * TILE
EPS = 1e-06
LOG2E = 1.4426950408889634
SCALE = HD**-0.5
OFF = -1e30

f32 = jnp.float32
bf16 = jnp.bfloat16


def dot(a, b, dims=((1,), (0,))):
    return lax.dot_general(a, b, (dims, ((), ())), preferred_element_type=f32)


def iota(shape, axis):
    return lax.broadcasted_iota(jnp.int32, shape, axis)


def head_sums(x, ones):
    high = x.astype(bf16)
    low = (x - high.astype(f32)).astype(bf16)
    return dot(high, ones) + dot(low, ones)


def normalize(x, gain, ones):
    wide = x.astype(f32)
    scale = lax.rsqrt(head_sums(wide * wide, ones) * (1.0 / HD) + EPS)
    unit = wide * scale
    return unit, scale, (unit * gain).astype(bf16)


def norm_backward(grad_hat, unit, scale, gain, ones):
    grad_unit = grad_hat * gain
    inner = head_sums(grad_unit * unit, ones) * (1.0 / HD)
    return scale * (grad_unit - unit * inner)


def shifted_rows(row):
    rows = jnp.broadcast_to(row, (TILE, LANES))
    return pltpu.roll(rows, 0, 1, stride=1, stride_axis=0)


def diagonal_sums(block):
    parts = [block[0:8]]
    for i in range(8, TILE, 8):
        parts.append(pltpu.roll(block[i : i + 8], LANES - i, 1))
    while len(parts) > 1:
        parts = [parts[i] + parts[i + 1] for i in range(0, len(parts), 2)]
    block = parts[0]
    index = iota((8, LANES), 0)
    for bit in (1, 2, 4):
        block = jnp.where((index & bit) != 0, pltpu.roll(block, LANES - bit, 1), block)
    return jnp.sum(block, axis=0, keepdims=True)


def tree_sum(parts):
    while len(parts) > 1:
        odd = parts[len(parts) // 2 * 2 :]
        parts = [parts[i] + parts[i + 1] for i in range(0, len(parts) - 1, 2)] + odd
    return parts[0]


def both_heads(a):
    first = iota((TILE, LANES), 1) < HD
    zero = jnp.zeros((), a.dtype)
    return jnp.concatenate([jnp.where(first, a, zero), jnp.where(first, zero, a)], axis=0)


def body(
    sizes,
    q_hbm,
    k_hbm,
    v_hbm,
    g_hbm,
    qgain_hbm,
    kgain_hbm,
    bias_hbm,
    dq_ref,
    dk_ref,
    dv_ref,
    dqgain_ref,
    dkgain_ref,
    dbias_ref,
    qgain_ref,
    kgain_ref,
    bias_ref,
    kv_ref,
    hkv_ref,
    qg_ref,
    nqg_ref,
    send_stat,
    recv_stat,
    unit_q,
    scale_q,
    unit_k,
    scale_k,
    dk_acc,
    khat_ref,
    k_ref,
    v_ref,
    qm_ref,
    gm_ref,
    qmn_ref,
    gmn_ref,
    e_ref,
    d_ref,
    low_ref,
    en_ref,
    dn_ref,
    pown_ref,
    pn_ref,
    sn_ref,
    abuf,
    again,
    asend,
    gain_yx,
    bbuf,
    cbuf,
    zgain,
    load_sem,
    halo_recv,
    halo_send,
    stat_sem,
    a_sem,
    b_sem,
    c_sem,
    level,
):
    nz, ny, nx, nc = sizes
    nsp = nz * ny
    z, y, x, c = (lax.axis_index(a) for a in ("z", "y", "x", "c"))
    sp = z * ny + y
    after, before = lax.rem(sp + 1, nsp), lax.rem(sp + nsp - 1, nsp)

    def at_sp(i):
        return {"z": i // ny, "y": lax.rem(i, ny)}

    def both_ways(name, place, size, distance):
        return [
            {name: lax.rem(place + distance, size)},
            {name: lax.rem(place + (distance // size + 1) * size - distance, size)},
        ]

    def tell(sem, targets):
        for target in targets:
            pl.semaphore_signal(sem, inc=1, device_id=target, device_id_type=MESH)

    def wait_bytes(ref, sem):
        pltpu.make_async_copy(ref, ref, sem).wait()

    lead = nc - 1
    at_lead = c == lead
    axes = both_ways("z", z, nz, 1) + both_ways("y", y, ny, 1)
    if nx > 1:
        axes += both_ways("x", x, nx, 1)
    partner = [{"c": lax.rem(c + d, nc)} for d in range(1, nc)]
    x_peers = [{"x": lax.rem(x + d, nx)} for d in range(1, nx)]
    two_away = both_ways("z", z, nz, 2) + both_ways("y", y, ny, 2)
    four_away = both_ways("z", z, nz, 4)
    level_1, level_2, level_3, x_ready, c_ready, z_ready, link_free = (
        level.at[i] for i in range(7)
    )

    barrier = pltpu.get_barrier_semaphore()
    neighbours = [at_sp(before), at_sp(after)] + axes + partner
    tell(barrier, neighbours)

    tiles = [slice(t * TILE, (t + 1) * TILE) for t in range(TILES)]
    wides = [slice(t * WIDE, (t + 1) * WIDE) for t in range(TILES)]
    small = [
        pltpu.make_async_copy(src, dst, load_sem.at[3 + i])
        for i, (src, dst) in enumerate(
            ((kgain_hbm, kgain_ref), (qgain_hbm, qgain_ref), (bias_hbm, bias_ref))
        )
    ]
    load_keys = pltpu.make_async_copy(k_hbm, k_ref, load_sem.at[0])
    load_keys.start()
    for load in small:
        load.start()
    for t in reversed(range(TILES)):
        dst = kv_ref.at[t, pl.ds(TILE, TILE)]
        pltpu.make_async_copy(v_hbm.at[tiles[t]], dst, load_sem.at[1]).start()
    for t in reversed(range(TILES)):
        for half, src in enumerate((q_hbm, g_hbm)):
            dst = qg_ref.at[t, pl.ds(half * TILE, TILE)]
            pltpu.make_async_copy(src.at[tiles[t]], dst, load_sem.at[2]).start()

    ones = (iota((LANES, LANES), 0) // HD == iota((LANES, LANES), 1) // HD).astype(bf16)
    small[0].wait()
    kgain = jnp.concatenate([kgain_ref[...], kgain_ref[...]], axis=1)
    load_keys.wait()
    for t in reversed(range(TILES)):
        unit, scale, hat = normalize(k_ref[tiles[t]], kgain, ones)
        unit_k[tiles[t]] = unit
        scale_k[tiles[t]] = scale
        khat_ref[tiles[t]] = hat
        kv_ref[t, 0:TILE] = hat
    pl.semaphore_wait(barrier, len(neighbours))

    def halo_copy(kind, tile):
        src, dst, to, recv = (
            (kv_ref, hkv_ref, after, tile),
            (qg_ref, nqg_ref, before, TILES),
        )[kind]
        return pltpu.make_async_remote_copy(
            src_ref=src.at[tile],
            dst_ref=dst.at[tile],
            send_sem=halo_send.at[2 if kind == 0 and tile < TILES - 1 else kind],
            recv_sem=halo_recv.at[recv],
            device_id=at_sp(to),
            device_id_type=MESH,
        )

    wait_bytes(v_ref, load_sem.at[1])
    halo_copy(0, TILES - 1).start()

    @pl.when(jnp.logical_not(at_lead))
    def _():
        for tile in reversed(range(TILES - 1)):
            halo_copy(0, tile).start()

    wait_bytes(qg_ref, load_sem.at[2])
    for tile in reversed(range(TILES)):
        halo_copy(1, tile).start()
    tell(level_1, axes)
    for load in small[1:]:
        load.wait()

    qgain = jnp.concatenate([qgain_ref[...], qgain_ref[...]], axis=1)

    key_i, query_i = iota((TILE, TILE), 0), iota((TILE, TILE), 1)
    reached = query_i >= key_i
    near, mid, far = [], [], []
    for h in range(2):
        row = bias_ref[h : h + 1, 0:LANES] * LOG2E
        last = bias_ref[h : h + 1, LANES : LANES + 1] * LOG2E
        table = shifted_rows(row)
        near.append(jnp.where(reached, table, OFF))
        mid.append(jnp.where(reached, last, table))
        far.append(jnp.broadcast_to(last, (1, TILE)))
    near = jnp.concatenate(near, axis=1)
    mid = jnp.concatenate(mid, axis=1)
    far = jnp.concatenate(far, axis=1)
    both_reached = jnp.concatenate([reached, reached], axis=1)
    wide_q = lax.rem(iota((TILE, WIDE), 1), TILE) // HD
    wide_k = iota((TILE, WIDE), 0) // HD
    edge = jnp.where(wide_k >= wide_q, 0.0, OFF)
    halo_off = jnp.where(sp > 0, 0.0, OFF)
    next_off = jnp.where(sp < nsp - 1, 0.0, OFF)

    def own_bias(distance):
        return (near, mid, far)[min(distance, 2)]

    def halo_bias(distance, off):
        if distance == 0:
            return far + edge + off
        return (mid if distance == TILES - 1 else far) + off

    for t in range(TILES):
        unit, scale, hat = normalize(qg_ref[t, 0:TILE], qgain, ones)
        unit_q[tiles[t]] = unit
        scale_q[tiles[t]] = scale
        qm_ref[wides[t]] = both_heads(hat)
        gm_ref[wides[t]] = both_heads(qg_ref[t, TILE:])
        v_ref[tiles[t]] = kv_ref[t, TILE:]

    nt = ((1,), (1,))
    l_parts, n_parts = [], []
    for t in range(TILES):
        count = (t + 1) * TILE
        s = dot(khat_ref[0:count], qm_ref[wides[t]], nt)
        d = dot(v_ref[0:count], gm_ref[wides[t]], nt)
        l_sum = jnp.zeros((1, WIDE), f32)
        n_sum = jnp.zeros((1, WIDE), f32)
        for ck in range(t + 1):
            part = tiles[ck]
            slot = slice((TILES - t + ck) * TILE, (TILES - t + ck + 1) * TILE)
            e = jnp.exp2(s[part] * (SCALE * LOG2E) + own_bias(t - ck))
            e_ref[t, slot] = e
            d_ref[t, slot] = d[part]
            l_sum += jnp.sum(e, axis=0, keepdims=True)
            n_sum += jnp.sum(e * d[part], axis=0, keepdims=True)
        l_parts.append(l_sum)
        n_parts.append(n_sum)
    pl.semaphore_wait(level_1, len(axes))
    tell(level_2, two_away)

    @pl.when(jnp.logical_not(at_lead))
    def _():
        wait_bytes(kv_ref.at[TILES - 1], halo_send.at[0])
        tell(link_free, [{"c": lead}])

    @pl.when(at_lead)
    def _():
        pl.semaphore_wait(link_free, 1)
        for tile in reversed(range(TILES - 1)):
            halo_copy(0, tile).start()

    def stat_copy(t):
        return pltpu.make_async_remote_copy(
            src_ref=send_stat.at[t],
            dst_ref=recv_stat.at[t],
            send_sem=stat_sem.at[0],
            recv_sem=stat_sem.at[1],
            device_id=at_sp(before),
            device_id_type=MESH,
        )

    def keys_of(t):
        halo = [hkv_ref[ck, 0:TILE] for ck in range(t, TILES)]
        return jnp.concatenate(halo + [khat_ref[0 : (t + 1) * TILE]], axis=0)

    def key_side(t):
        own = (TILES - t) * TILE
        dk_t = dot(low_ref[t], qm_ref[wides[t]])
        if t == TILES - 1:
            dk_acc[...] = dk_t[own:]
        else:
            dk_acc[0 : (t + 1) * TILE] += dk_t[own:]
        return jnp.sum(dk_t * keys_of(t).astype(f32), axis=0, keepdims=True)

    total = jnp.zeros((1, WIDE), f32)
    near_sum = jnp.zeros((TILE, WIDE), f32)
    mid_sum = jnp.zeros((TILE, WIDE), f32)
    gain_sum = jnp.zeros((1, LANES), f32)
    for ck in reversed(range(TILES)):
        wait_bytes(hkv_ref.at[ck], halo_recv.at[ck])
        if ck == TILES - 1:
            pl.semaphore_wait(level_2, len(two_away))
            tell(level_3, four_away)
            tell(x_ready, x_peers)
        if ck == 0:

            @pl.when(at_lead)
            def _():
                pl.semaphore_wait(x_ready, len(x_peers))
                tell(c_ready, partner)

        if ck < TILES - 1:
            gain_sum += key_side(ck + 1)
        span = (ck + 1) * WIDE
        s = dot(hkv_ref[ck, 0:TILE], qm_ref[0:span], nt)
        d = dot(hkv_ref[ck, TILE:], gm_ref[0:span], nt)
        for t in reversed(range(ck + 1)):
            part = wides[t]
            slot = slice((ck - t) * TILE, (ck - t + 1) * TILE)
            e = jnp.exp2(s[:, part] * (SCALE * LOG2E) + halo_bias(ck - t, halo_off))
            e_ref[t, slot] = e
            d_ref[t, slot] = d[:, part]
            l_parts[t] += jnp.sum(e, axis=0, keepdims=True)
            n_parts[t] += jnp.sum(e * d[:, part], axis=0, keepdims=True)
        t = ck
        inv = 1.0 / l_parts[t]
        delta = n_parts[t] * inv
        send_stat[t, 0:1] = inv
        send_stat[t, 1:2] = delta
        prob = e_ref[t] * inv
        grad = prob * (d_ref[t] - delta)
        total += jnp.sum(grad, axis=0, keepdims=True)
        own = (TILES - t) * TILE
        near_sum += grad[TILES * TILE :]
        mid_sum += grad[(TILES - 1) * TILE : TILES * TILE]
        low = grad.astype(bf16)
        low_ref[t] = low

    gain_sum += key_side(0)

    diagonals = jnp.where(both_reached, near_sum, mid_sum)
    taps = [diagonal_sums(diagonals[:, h * TILE : (h + 1) * TILE]) for h in range(2)]
    folded = [total[:, h * TILE : (h + 1) * TILE] for h in range(2)]
    folded = [part + pltpu.roll(part, HD, 1) for part in folded]
    first_half = iota((1, LANES), 1) < HD
    sums = jnp.where(first_half, folded[0], folded[1])
    asend[...] = gain_sum
    abuf[y] = jnp.concatenate([taps[0], taps[1], sums, gain_sum], axis=0)

    group = ny * nx
    others = [(dy, dx) for dx in range(nx) for dy in range(ny)][1:]
    others.sort(key=lambda o: -min(o[0], ny - o[0]) - min(o[1], nx - o[1]))
    y_others = sorted(range(1, ny), key=lambda d: -min(d, ny - d))
    z_others = sorted(range(1, nz), key=lambda d: -min(d, nz - d))

    def gain_copy(dy, dx):
        return pltpu.make_async_remote_copy(
            src_ref=asend,
            dst_ref=again.at[c * group + x * ny + y],
            send_sem=a_sem.at[1],
            recv_sem=a_sem.at[3],
            device_id={"y": lax.rem(y + dy, ny), "x": lax.rem(x + dx, nx), "c": lead},
            device_id_type=MESH,
        )

    def a_copy(dy):
        return pltpu.make_async_remote_copy(
            src_ref=abuf.at[y],
            dst_ref=abuf.at[y],
            send_sem=a_sem.at[0],
            recv_sem=a_sem.at[2],
            device_id={"y": lax.rem(y + dy, ny)},
            device_id_type=MESH,
        )

    @pl.when(jnp.logical_not(at_lead))
    def _():
        pl.semaphore_wait(x_ready, len(x_peers))
        pl.semaphore_wait(c_ready, 1)

    for dy, dx in others:
        gain_copy(dy, dx).start()

    @pl.when(jnp.logical_not(at_lead))
    def _():
        gain_copy(0, 0).start()

    for dy in y_others:
        a_copy(dy).start()
    for t in range(TILES):
        stat_copy(t).start()

    wait_bytes(nqg_ref, halo_recv.at[TILES])
    for t in reversed(range(TILES)):
        qmn_ref[wides[t]] = both_heads(normalize(nqg_ref[t, 0:TILE], qgain, ones)[2])
        gmn_ref[wides[t]] = both_heads(nqg_ref[t, TILE:])
        s = dot(khat_ref[t * TILE :], qmn_ref[wides[t]], nt)
        d = dot(v_ref[t * TILE :], gmn_ref[wides[t]], nt)
        for ck in range(t, TILES):
            part = slice((ck - t) * TILE, (ck - t + 1) * TILE)
            en_ref[tiles[ck], wides[t]] = jnp.exp2(
                s[part] * (SCALE * LOG2E) + halo_bias(ck - t, next_off)
            )
            dn_ref[tiles[ck], wides[t]] = d[part]

    pl.semaphore_wait(level_3, len(four_away))

    @pl.when(jnp.logical_not(at_lead))
    def _():
        tell(z_ready, [{"c": lead}])

    for t in range(TILES):
        rows = tiles[t]
        own = (TILES - t) * TILE
        prob = e_ref[t, own:] * send_stat[t, 0:1]
        pown_ref[0 : (t + 1) * TILE, wides[t]] = prob.astype(bf16)
        keys = keys_of(t)
        dq_t = dot(keys, low_ref[t], ((0,), (0,)))
        dq_t = jnp.concatenate([dq_t[0:HD, 0:TILE], dq_t[HD:, TILE:]], axis=0) * SCALE
        dq_ref[rows] = norm_backward(
            dq_t.T, unit_q[rows], scale_q[rows], qgain, ones
        ).astype(bf16)

    @pl.when(at_lead)
    def _():
        wait_bytes(again.at[pl.ds(0, nc * group - 1)], a_sem.at[3])
        again[c * group + x * ny + y] = asend[...]
        gain_yx[...] = tree_sum([again[i] for i in range(nc * group)])

    wait_bytes(abuf.at[pl.ds(0, ny - 1)], a_sem.at[2])
    block = tree_sum([abuf[i] for i in range(ny)])
    bbuf[z] = block

    @pl.when(at_lead)
    def _():
        bbuf[z, 3:4] = gain_yx[...]

    def b_copy(dz):
        return pltpu.make_async_remote_copy(
            src_ref=bbuf.at[z],
            dst_ref=bbuf.at[z],
            send_sem=b_sem.at[0],
            recv_sem=b_sem.at[1],
            device_id={"z": lax.rem(z + dz, nz)},
            device_id_type=MESH,
        )

    def down_copy(dz):
        return pltpu.make_async_remote_copy(
            src_ref=gain_yx,
            dst_ref=zgain.at[z],
            send_sem=c_sem.at[0],
            recv_sem=c_sem.at[1],
            device_id={"z": lax.rem(z + dz, nz), "c": 0},
            device_id_type=MESH,
        )

    for dz in z_others:
        b_copy(dz).start()

    @pl.when(at_lead)
    def _():
        pl.semaphore_wait(z_ready, 1)
        for dz in z_others + [0]:
            down_copy(dz).start()

    wait_bytes(recv_stat, stat_sem.at[1])
    for t in reversed(range(TILES)):
        inv, delta = recv_stat[t, 0:1], recv_stat[t, 1:2]
        prob = en_ref[t * TILE :, wides[t]] * inv
        pn_ref[t * TILE :, wides[t]] = prob.astype(bf16)
        sn_ref[t * TILE :, wides[t]] = (prob * (dn_ref[t * TILE :, wides[t]] - delta)).astype(bf16)

    for ck in range(TILES):
        rows = tiles[ck]
        own, later = slice(ck * WIDE, TILES * WIDE), slice(0, (ck + 1) * WIDE)
        dv = dot(pown_ref[rows, own], gm_ref[own]) + dot(pn_ref[rows, later], gmn_ref[later])
        dv_ref[rows] = dv.astype(bf16)
        dk = dk_acc[rows] + dot(sn_ref[rows, later], qmn_ref[later])
        dk_ref[rows] = norm_backward(
            dk * SCALE, unit_k[rows], scale_k[rows], kgain, ones
        ).astype(bf16)

    wait_bytes(qg_ref, halo_send.at[1])
    wait_bytes(kv_ref.at[pl.ds(0, TILES - 1)], halo_send.at[2])
    wait_bytes(send_stat, stat_sem.at[0])
    wait_bytes(abuf.at[pl.ds(0, ny - 1)], a_sem.at[0])

    @pl.when(at_lead)
    def _():
        wait_bytes(kv_ref.at[TILES - 1], halo_send.at[0])
        wait_bytes(again.at[pl.ds(0, group - 1)], a_sem.at[1])

    @pl.when(jnp.logical_not(at_lead))
    def _():
        wait_bytes(again.at[pl.ds(0, group)], a_sem.at[1])

    wait_bytes(bbuf.at[pl.ds(0, nz - 1)], b_sem.at[1])
    block = tree_sum([bbuf[i] for i in range(nz)])

    @pl.when(at_lead)
    def _():
        cbuf[...] = block[3:4]

    @pl.when(jnp.logical_not(at_lead))
    def _():
        wait_bytes(zgain, c_sem.at[1])
        cbuf[...] = tree_sum([zgain[i] for i in range(nz)])

    for h in range(2):
        taps = block[h : h + 1]
        rest = jnp.where(first_half if h == 0 else ~first_half, block[2:3], 0.0) - taps
        dbias_ref[h : h + 1, 0:LANES] = taps
        dbias_ref[h : h + 1, LANES : LANES + 1] = jnp.sum(rest, axis=1, keepdims=True)

    gain_sum = cbuf[...]
    gain_sum = (gain_sum + pltpu.roll(gain_sum, HD, 1))[:, 0:HD] * SCALE
    dqgain_ref[...] = gain_sum / qgain_ref[...]
    dkgain_ref[...] = gain_sum / kgain_ref[...]
    wait_bytes(bbuf.at[pl.ds(0, nz - 1)], b_sem.at[0])

    @pl.when(at_lead)
    def _():
        wait_bytes(zgain, c_sem.at[0])


def flush(*refs):
    count = len(refs) // 2
    sems = refs[-1]
    copies = [
        pltpu.make_async_copy(refs[i], refs[count + i], sems.at[i]) for i in range(count)
    ]
    for copy in copies:
        copy.start()
    for copy in copies:
        copy.wait()


def per_device(sizes, query, key, value, out_grad, query_gain, key_gain, rel_bias):
    nz, ny, nx, nc = sizes
    vmem = pl.BlockSpec(memory_space=pltpu.VMEM)
    hbm = pl.BlockSpec(memory_space=pl.ANY)
    dma = pltpu.SemaphoreType.DMA
    regular = pltpu.SemaphoreType.REGULAR
    shapes = (((ROWS, LANES), bf16),) * 3 + (((1, HD), f32),) * 2 + ((rel_bias.shape, f32),)
    tile_rows, wide_rows = (ROWS, LANES), (TILES * WIDE, LANES)
    square = (ROWS, TILES * WIDE)
    outs = pl.pallas_call(
        functools.partial(body, sizes),
        out_shape=tuple(pltpu.VMEM(*s) for s in shapes),
        in_specs=[hbm] * 7,
        out_specs=(vmem,) * 6,
        scratch_shapes=[
            *[pltpu.VMEM((1, HD), f32)] * 2,
            pltpu.VMEM(rel_bias.shape, f32),
            *[pltpu.VMEM((TILES, 2 * TILE, LANES), bf16)] * 4,
            *[pltpu.VMEM((TILES, 2, WIDE), f32)] * 2,
            *[pltpu.VMEM(tile_rows, f32)] * 5,
            *[pltpu.VMEM(tile_rows, bf16)] * 3,
            *[pltpu.VMEM(wide_rows, bf16)] * 4,
            *[pltpu.VMEM((TILES, (TILES + 1) * TILE, WIDE), f32)] * 2,
            pltpu.VMEM((TILES, (TILES + 1) * TILE, WIDE), bf16),
            *[pltpu.VMEM(square, f32)] * 2,
            *[pltpu.VMEM(square, bf16)] * 3,
            pltpu.VMEM((ny, 4, LANES), f32),
            pltpu.VMEM((nc * nx * ny, 1, LANES), f32),
            pltpu.VMEM((1, LANES), f32),
            pltpu.VMEM((1, LANES), f32),
            pltpu.VMEM((nz, 4, LANES), f32),
            pltpu.VMEM((1, LANES), f32),
            pltpu.VMEM((nz, 1, LANES), f32),
            dma((6,)),
            dma((TILES + 1,)),
            dma((3,)),
            dma((2,)),
            dma((4,)),
            dma((2,)),
            dma((2,)),
            regular((7,)),
        ],
        compiler_params=pltpu.CompilerParams(collective_id=0, has_side_effects=True),
        name="segment_backward",
    )(query, key, value, out_grad, query_gain.reshape(1, HD), key_gain.reshape(1, HD), rel_bias)
    outs = pl.pallas_call(
        flush,
        out_shape=tuple(jax.ShapeDtypeStruct(*s) for s in shapes),
        in_specs=[vmem] * 6,
        out_specs=(hbm,) * 6,
        scratch_shapes=[dma((6,))],
        name="flush",
    )(*(pltpu.with_memory_space_constraint(o, pltpu.VMEM) for o in outs))
    return (*outs[:3], outs[3].reshape(HD), outs[4].reshape(HD), outs[5])


def solution(mesh):
    sizes = mesh_sizes(mesh)
    torus = Mesh(mesh.devices.reshape(sizes), ("z", "y", "x", "c"))
    return jax.shard_map(
        functools.partial(per_device, sizes),
        mesh=torus,
        in_specs=(P(SP, TP), P(SP, TP), P(SP, TP), P(SP, TP), P(), P(), P(TP, None)),
        out_specs=(P(SP, TP), P(SP, TP), P(SP, TP), P(), P(), P(TP, None)),
        check_vma=False,
    )


def mesh_sizes(mesh):
    return (16, 8, 4, 2)
```

```python
import functools

import jax
import jax.numpy as jnp
from jax import lax
from jax.experimental import pallas as pl
from jax.experimental.pallas import tpu as pltpu
from jax.sharding import Mesh
from jax.sharding import PartitionSpec as P

SP = ("z", "y")
TP = ("x", "c")
MESH = pl.DeviceIdType.MESH

ROWS = 512
TILE = 128
TILES = ROWS // TILE
LANES = 128
HD = 64
WIDE = 2 * TILE
EPS = 1e-06
LOG2E = 1.4426950408889634
SCALE = HD**-0.5
OFF = -1e30

f32 = jnp.float32
bf16 = jnp.bfloat16


def dot(a, b, dims=((1,), (0,))):
    return lax.dot_general(a, b, (dims, ((), ())), preferred_element_type=f32)


def iota(shape, axis):
    return lax.broadcasted_iota(jnp.int32, shape, axis)


def head_sums(x, ones):
    high = x.astype(bf16)
    low = (x - high.astype(f32)).astype(bf16)
    return dot(high, ones) + dot(low, ones)


def normalize(x, gain, ones):
    wide = x.astype(f32)
    scale = lax.rsqrt(head_sums(wide * wide, ones) * (1.0 / HD) + EPS)
    unit = wide * scale
    return unit, scale, (unit * gain).astype(bf16)


def norm_backward(grad_hat, unit, scale, gain, ones):
    grad_unit = grad_hat * gain
    inner = head_sums(grad_unit * unit, ones) * (1.0 / HD)
    return scale * (grad_unit - unit * inner)


def shifted_rows(row):
    rows = jnp.broadcast_to(row, (TILE, LANES))
    return pltpu.roll(rows, 0, 1, stride=1, stride_axis=0)


def diagonal_sums(block):
    parts = [block[0:8]]
    for i in range(8, TILE, 8):
        parts.append(pltpu.roll(block[i : i + 8], LANES - i, 1))
    while len(parts) > 1:
        parts = [parts[i] + parts[i + 1] for i in range(0, len(parts), 2)]
    block = parts[0]
    index = iota((8, LANES), 0)
    for bit in (1, 2, 4):
        block = jnp.where((index & bit) != 0, pltpu.roll(block, LANES - bit, 1), block)
    return jnp.sum(block, axis=0, keepdims=True)


def tree_sum(parts):
    while len(parts) > 1:
        odd = parts[len(parts) // 2 * 2 :]
        parts = [parts[i] + parts[i + 1] for i in range(0, len(parts) - 1, 2)] + odd
    return parts[0]


def both_heads(a):
    first = iota((TILE, LANES), 1) < HD
    zero = jnp.zeros((), a.dtype)
    return jnp.concatenate([jnp.where(first, a, zero), jnp.where(first, zero, a)], axis=0)


def body(
    sizes,
    q_hbm,
    k_hbm,
    v_hbm,
    g_hbm,
    qgain_hbm,
    kgain_hbm,
    bias_hbm,
    dq_ref,
    dk_ref,
    dv_ref,
    dqgain_ref,
    dkgain_ref,
    dbias_ref,
    qgain_ref,
    kgain_ref,
    bias_ref,
    kv_ref,
    hkv_ref,
    qg_ref,
    nqg_ref,
    send_stat,
    recv_stat,
    unit_q,
    scale_q,
    unit_k,
    scale_k,
    dk_acc,
    khat_ref,
    k_ref,
    v_ref,
    qm_ref,
    gm_ref,
    qmn_ref,
    gmn_ref,
    e_ref,
    d_ref,
    low_ref,
    en_ref,
    dn_ref,
    pown_ref,
    pn_ref,
    sn_ref,
    abuf,
    again,
    asend,
    gain_yx,
    bbuf,
    cbuf,
    zgain,
    load_sem,
    halo_recv,
    halo_send,
    stat_sem,
    a_sem,
    b_sem,
    c_sem,
    level,
):
    nz, ny, nx, nc = sizes
    nsp = nz * ny
    z, y, x, c = (lax.axis_index(a) for a in ("z", "y", "x", "c"))
    sp = z * ny + y
    after, before = lax.rem(sp + 1, nsp), lax.rem(sp + nsp - 1, nsp)

    def at_sp(i):
        return {"z": i // ny, "y": lax.rem(i, ny)}

    def both_ways(name, place, size, distance):
        return [
            {name: lax.rem(place + distance, size)},
            {name: lax.rem(place + (distance // size + 1) * size - distance, size)},
        ]

    def tell(sem, targets):
        for target in targets:
            pl.semaphore_signal(sem, inc=1, device_id=target, device_id_type=MESH)

    def wait_bytes(ref, sem):
        pltpu.make_async_copy(ref, ref, sem).wait()

    lead = nc - 1
    at_lead = c == lead
    axes = both_ways("z", z, nz, 1) + both_ways("y", y, ny, 1)
    if nx > 1:
        axes += both_ways("x", x, nx, 1)
    partner = [{"c": lax.rem(c + d, nc)} for d in range(1, nc)]
    x_peers = [{"x": lax.rem(x + d, nx)} for d in range(1, nx)]
    two_away = both_ways("z", z, nz, 2) + both_ways("y", y, ny, 2)
    four_away = both_ways("z", z, nz, 4)
    level_1, level_2, level_3, x_ready, c_ready, z_ready, link_free = (
        level.at[i] for i in range(7)
    )

    barrier = pltpu.get_barrier_semaphore()
    neighbours = [at_sp(before), at_sp(after)] + axes + partner
    tell(barrier, neighbours)

    tiles = [slice(t * TILE, (t + 1) * TILE) for t in range(TILES)]
    wides = [slice(t * WIDE, (t + 1) * WIDE) for t in range(TILES)]
    small = [
        pltpu.make_async_copy(src, dst, load_sem.at[3 + i])
        for i, (src, dst) in enumerate(
            ((kgain_hbm, kgain_ref), (qgain_hbm, qgain_ref), (bias_hbm, bias_ref))
        )
    ]
    load_keys = pltpu.make_async_copy(k_hbm, k_ref, load_sem.at[0])
    load_keys.start()
    for load in small:
        load.start()
    for t in reversed(range(TILES)):
        dst = kv_ref.at[t, pl.ds(TILE, TILE)]
        pltpu.make_async_copy(v_hbm.at[tiles[t]], dst, load_sem.at[1]).start()
    for t in reversed(range(TILES)):
        for half, src in enumerate((q_hbm, g_hbm)):
            dst = qg_ref.at[t, pl.ds(half * TILE, TILE)]
            pltpu.make_async_copy(src.at[tiles[t]], dst, load_sem.at[2]).start()

    ones = (iota((LANES, LANES), 0) // HD == iota((LANES, LANES), 1) // HD).astype(bf16)
    small[0].wait()
    kgain = jnp.concatenate([kgain_ref[...], kgain_ref[...]], axis=1)
    load_keys.wait()
    for t in reversed(range(TILES)):
        unit, scale, hat = normalize(k_ref[tiles[t]], kgain, ones)
        unit_k[tiles[t]] = unit
        scale_k[tiles[t]] = scale
        khat_ref[tiles[t]] = hat
        kv_ref[t, 0:TILE] = hat
    pl.semaphore_wait(barrier, len(neighbours))

    def halo_copy(kind, tile):
        src, dst, to, recv = (
            (kv_ref, hkv_ref, after, tile),
            (qg_ref, nqg_ref, before, TILES),
        )[kind]
        return pltpu.make_async_remote_copy(
            src_ref=src.at[tile],
            dst_ref=dst.at[tile],
            send_sem=halo_send.at[2 if kind == 0 and tile < TILES // 2 else kind],
            recv_sem=halo_recv.at[recv],
            device_id=at_sp(to),
            device_id_type=MESH,
        )

    wait_bytes(v_ref, load_sem.at[1])
    halo_copy(0, TILES - 1).start()

    @pl.when(jnp.logical_not(at_lead))
    def _():
        for tile in reversed(range(TILES - 1)):
            halo_copy(0, tile).start()

    wait_bytes(qg_ref, load_sem.at[2])
    for tile in reversed(range(TILES)):
        halo_copy(1, tile).start()
    tell(level_1, axes)
    for load in small[1:]:
        load.wait()

    qgain = jnp.concatenate([qgain_ref[...], qgain_ref[...]], axis=1)

    key_i, query_i = iota((TILE, TILE), 0), iota((TILE, TILE), 1)
    reached = query_i >= key_i
    near, mid, far = [], [], []
    for h in range(2):
        row = bias_ref[h : h + 1, 0:LANES] * LOG2E
        last = bias_ref[h : h + 1, LANES : LANES + 1] * LOG2E
        table = shifted_rows(row)
        near.append(jnp.where(reached, table, OFF))
        mid.append(jnp.where(reached, last, table))
        far.append(jnp.broadcast_to(last, (1, TILE)))
    near = jnp.concatenate(near, axis=1)
    mid = jnp.concatenate(mid, axis=1)
    far = jnp.concatenate(far, axis=1)
    both_reached = jnp.concatenate([reached, reached], axis=1)
    wide_q = lax.rem(iota((TILE, WIDE), 1), TILE) // HD
    wide_k = iota((TILE, WIDE), 0) // HD
    edge = jnp.where(wide_k >= wide_q, 0.0, OFF)
    halo_off = jnp.where(sp > 0, 0.0, OFF)
    next_off = jnp.where(sp < nsp - 1, 0.0, OFF)

    def own_bias(distance):
        return (near, mid, far)[min(distance, 2)]

    def halo_bias(distance, off):
        if distance == 0:
            return far + edge + off
        return (mid if distance == TILES - 1 else far) + off

    for t in range(TILES):
        unit, scale, hat = normalize(qg_ref[t, 0:TILE], qgain, ones)
        unit_q[tiles[t]] = unit
        scale_q[tiles[t]] = scale
        qm_ref[wides[t]] = both_heads(hat)
        gm_ref[wides[t]] = both_heads(qg_ref[t, TILE:])
        v_ref[tiles[t]] = kv_ref[t, TILE:]

    nt = ((1,), (1,))
    l_parts, n_parts = [], []
    for t in range(TILES):
        count = (t + 1) * TILE
        s = dot(khat_ref[0:count], qm_ref[wides[t]], nt)
        d = dot(v_ref[0:count], gm_ref[wides[t]], nt)
        l_sum = jnp.zeros((1, WIDE), f32)
        n_sum = jnp.zeros((1, WIDE), f32)
        for ck in range(t + 1):
            part = tiles[ck]
            slot = slice((TILES - t + ck) * TILE, (TILES - t + ck + 1) * TILE)
            e = jnp.exp2(s[part] * (SCALE * LOG2E) + own_bias(t - ck))
            e_ref[t, slot] = e
            d_ref[t, slot] = d[part]
            l_sum += jnp.sum(e, axis=0, keepdims=True)
            n_sum += jnp.sum(e * d[part], axis=0, keepdims=True)
        l_parts.append(l_sum)
        n_parts.append(n_sum)
    pl.semaphore_wait(level_1, len(axes))
    tell(level_2, two_away)

    @pl.when(jnp.logical_not(at_lead))
    def _():
        wait_bytes(kv_ref.at[pl.ds(TILES // 2, TILES // 2)], halo_send.at[0])
        tell(link_free, [{"c": lead}])

    @pl.when(at_lead)
    def _():
        pl.semaphore_wait(link_free, 1)
        for tile in reversed(range(TILES - 1)):
            halo_copy(0, tile).start()

    def stat_copy(t):
        return pltpu.make_async_remote_copy(
            src_ref=send_stat.at[t],
            dst_ref=recv_stat.at[t],
            send_sem=stat_sem.at[0],
            recv_sem=stat_sem.at[1],
            device_id=at_sp(before),
            device_id_type=MESH,
        )

    def keys_of(t):
        halo = [hkv_ref[ck, 0:TILE] for ck in range(t, TILES)]
        return jnp.concatenate(halo + [khat_ref[0 : (t + 1) * TILE]], axis=0)

    def key_side(t):
        own = (TILES - t) * TILE
        dk_t = dot(low_ref[t], qm_ref[wides[t]])
        if t == TILES - 1:
            dk_acc[...] = dk_t[own:]
        else:
            dk_acc[0 : (t + 1) * TILE] += dk_t[own:]
        return jnp.sum(dk_t * keys_of(t).astype(f32), axis=0, keepdims=True)

    total = jnp.zeros((1, WIDE), f32)
    near_sum = jnp.zeros((TILE, WIDE), f32)
    mid_sum = jnp.zeros((TILE, WIDE), f32)
    gain_sum = jnp.zeros((1, LANES), f32)
    for ck in reversed(range(TILES)):
        wait_bytes(hkv_ref.at[ck], halo_recv.at[ck])
        if ck == TILES - 1:
            pl.semaphore_wait(level_2, len(two_away))
            tell(level_3, four_away)
            tell(x_ready, x_peers)
        if ck == TILES - 2:

            @pl.when(at_lead)
            def _():
                pl.semaphore_wait(x_ready, len(x_peers))
                tell(c_ready, partner)

        if ck < TILES - 1:
            gain_sum += key_side(ck + 1)
        span = (ck + 1) * WIDE
        s = dot(hkv_ref[ck, 0:TILE], qm_ref[0:span], nt)
        d = dot(hkv_ref[ck, TILE:], gm_ref[0:span], nt)
        for t in reversed(range(ck + 1)):
            part = wides[t]
            slot = slice((ck - t) * TILE, (ck - t + 1) * TILE)
            e = jnp.exp2(s[:, part] * (SCALE * LOG2E) + halo_bias(ck - t, halo_off))
            e_ref[t, slot] = e
            d_ref[t, slot] = d[:, part]
            l_parts[t] += jnp.sum(e, axis=0, keepdims=True)
            n_parts[t] += jnp.sum(e * d[:, part], axis=0, keepdims=True)
        t = ck
        inv = 1.0 / l_parts[t]
        delta = n_parts[t] * inv
        send_stat[t, 0:1] = inv
        send_stat[t, 1:2] = delta
        prob = e_ref[t] * inv
        grad = prob * (d_ref[t] - delta)
        total += jnp.sum(grad, axis=0, keepdims=True)
        own = (TILES - t) * TILE
        near_sum += grad[TILES * TILE :]
        mid_sum += grad[(TILES - 1) * TILE : TILES * TILE]
        low = grad.astype(bf16)
        low_ref[t] = low

    gain_sum += key_side(0)

    diagonals = jnp.where(both_reached, near_sum, mid_sum)
    taps = [diagonal_sums(diagonals[:, h * TILE : (h + 1) * TILE]) for h in range(2)]
    folded = [total[:, h * TILE : (h + 1) * TILE] for h in range(2)]
    folded = [part + pltpu.roll(part, HD, 1) for part in folded]
    first_half = iota((1, LANES), 1) < HD
    sums = jnp.where(first_half, folded[0], folded[1])
    asend[...] = gain_sum
    abuf[y] = jnp.concatenate([taps[0], taps[1], sums, gain_sum], axis=0)

    group = ny * nx
    others = [(dy, dx) for dx in range(nx) for dy in range(ny)][1:]
    others.sort(key=lambda o: -min(o[0], ny - o[0]) - min(o[1], nx - o[1]))
    y_others = sorted(range(1, ny), key=lambda d: -min(d, ny - d))
    z_others = sorted(range(1, nz), key=lambda d: -min(d, nz - d))

    def gain_copy(dy, dx):
        return pltpu.make_async_remote_copy(
            src_ref=asend,
            dst_ref=again.at[c * group + x * ny + y],
            send_sem=a_sem.at[1],
            recv_sem=a_sem.at[3],
            device_id={"y": lax.rem(y + dy, ny), "x": lax.rem(x + dx, nx), "c": lead},
            device_id_type=MESH,
        )

    def a_copy(dy):
        return pltpu.make_async_remote_copy(
            src_ref=abuf.at[y],
            dst_ref=abuf.at[y],
            send_sem=a_sem.at[0],
            recv_sem=a_sem.at[2],
            device_id={"y": lax.rem(y + dy, ny)},
            device_id_type=MESH,
        )

    @pl.when(jnp.logical_not(at_lead))
    def _():
        pl.semaphore_wait(x_ready, len(x_peers))
        pl.semaphore_wait(c_ready, 1)

    for dy, dx in others:
        gain_copy(dy, dx).start()

    @pl.when(jnp.logical_not(at_lead))
    def _():
        gain_copy(0, 0).start()

    for dy in y_others:
        a_copy(dy).start()
    for t in range(TILES):
        stat_copy(t).start()

    wait_bytes(nqg_ref, halo_recv.at[TILES])
    for t in reversed(range(TILES)):
        qmn_ref[wides[t]] = both_heads(normalize(nqg_ref[t, 0:TILE], qgain, ones)[2])
        gmn_ref[wides[t]] = both_heads(nqg_ref[t, TILE:])
        s = dot(khat_ref[t * TILE :], qmn_ref[wides[t]], nt)
        d = dot(v_ref[t * TILE :], gmn_ref[wides[t]], nt)
        for ck in range(t, TILES):
            part = slice((ck - t) * TILE, (ck - t + 1) * TILE)
            en_ref[tiles[ck], wides[t]] = jnp.exp2(
                s[part] * (SCALE * LOG2E) + halo_bias(ck - t, next_off)
            )
            dn_ref[tiles[ck], wides[t]] = d[part]

    pl.semaphore_wait(level_3, len(four_away))

    @pl.when(jnp.logical_not(at_lead))
    def _():
        tell(z_ready, [{"c": lead}])

    for t in range(TILES):
        rows = tiles[t]
        own = (TILES - t) * TILE
        prob = e_ref[t, own:] * send_stat[t, 0:1]
        pown_ref[0 : (t + 1) * TILE, wides[t]] = prob.astype(bf16)
        keys = keys_of(t)
        dq_t = dot(keys, low_ref[t], ((0,), (0,)))
        dq_t = jnp.concatenate([dq_t[0:HD, 0:TILE], dq_t[HD:, TILE:]], axis=0) * SCALE
        dq_ref[rows] = norm_backward(
            dq_t.T, unit_q[rows], scale_q[rows], qgain, ones
        ).astype(bf16)

    @pl.when(at_lead)
    def _():
        wait_bytes(again.at[pl.ds(0, nc * group - 1)], a_sem.at[3])
        again[c * group + x * ny + y] = asend[...]
        gain_yx[...] = tree_sum([again[i] for i in range(nc * group)])

    wait_bytes(abuf.at[pl.ds(0, ny - 1)], a_sem.at[2])
    block = tree_sum([abuf[i] for i in range(ny)])
    bbuf[z] = block

    @pl.when(at_lead)
    def _():
        bbuf[z, 3:4] = gain_yx[...]

    def b_copy(dz):
        return pltpu.make_async_remote_copy(
            src_ref=bbuf.at[z],
            dst_ref=bbuf.at[z],
            send_sem=b_sem.at[0],
            recv_sem=b_sem.at[1],
            device_id={"z": lax.rem(z + dz, nz)},
            device_id_type=MESH,
        )

    def down_copy(dz):
        return pltpu.make_async_remote_copy(
            src_ref=gain_yx,
            dst_ref=zgain.at[z],
            send_sem=c_sem.at[0],
            recv_sem=c_sem.at[1],
            device_id={"z": lax.rem(z + dz, nz), "c": 0},
            device_id_type=MESH,
        )

    for dz in z_others:
        b_copy(dz).start()

    @pl.when(at_lead)
    def _():
        pl.semaphore_wait(z_ready, 1)
        for dz in z_others + [0]:
            down_copy(dz).start()

    wait_bytes(recv_stat, stat_sem.at[1])
    for t in reversed(range(TILES)):
        inv, delta = recv_stat[t, 0:1], recv_stat[t, 1:2]
        prob = en_ref[t * TILE :, wides[t]] * inv
        pn_ref[t * TILE :, wides[t]] = prob.astype(bf16)
        sn_ref[t * TILE :, wides[t]] = (prob * (dn_ref[t * TILE :, wides[t]] - delta)).astype(bf16)

    for ck in range(TILES):
        rows = tiles[ck]
        own, later = slice(ck * WIDE, TILES * WIDE), slice(0, (ck + 1) * WIDE)
        dv = dot(pown_ref[rows, own], gm_ref[own]) + dot(pn_ref[rows, later], gmn_ref[later])
        dv_ref[rows] = dv.astype(bf16)
        dk = dk_acc[rows] + dot(sn_ref[rows, later], qmn_ref[later])
        dk_ref[rows] = norm_backward(
            dk * SCALE, unit_k[rows], scale_k[rows], kgain, ones
        ).astype(bf16)

    wait_bytes(qg_ref, halo_send.at[1])
    wait_bytes(kv_ref.at[pl.ds(0, TILES // 2)], halo_send.at[2])
    wait_bytes(send_stat, stat_sem.at[0])
    wait_bytes(abuf.at[pl.ds(0, ny - 1)], a_sem.at[0])

    @pl.when(at_lead)
    def _():
        wait_bytes(kv_ref.at[pl.ds(TILES // 2, TILES // 2)], halo_send.at[0])
        wait_bytes(again.at[pl.ds(0, group - 1)], a_sem.at[1])

    @pl.when(jnp.logical_not(at_lead))
    def _():
        wait_bytes(again.at[pl.ds(0, group)], a_sem.at[1])

    wait_bytes(bbuf.at[pl.ds(0, nz - 1)], b_sem.at[1])
    block = tree_sum([bbuf[i] for i in range(nz)])

    @pl.when(at_lead)
    def _():
        cbuf[...] = block[3:4]

    @pl.when(jnp.logical_not(at_lead))
    def _():
        wait_bytes(zgain, c_sem.at[1])
        cbuf[...] = tree_sum([zgain[i] for i in range(nz)])

    for h in range(2):
        taps = block[h : h + 1]
        rest = jnp.where(first_half if h == 0 else ~first_half, block[2:3], 0.0) - taps
        dbias_ref[h : h + 1, 0:LANES] = taps
        dbias_ref[h : h + 1, LANES : LANES + 1] = jnp.sum(rest, axis=1, keepdims=True)

    gain_sum = cbuf[...]
    gain_sum = (gain_sum + pltpu.roll(gain_sum, HD, 1))[:, 0:HD] * SCALE
    dqgain_ref[...] = gain_sum / qgain_ref[...]
    dkgain_ref[...] = gain_sum / kgain_ref[...]
    wait_bytes(bbuf.at[pl.ds(0, nz - 1)], b_sem.at[0])

    @pl.when(at_lead)
    def _():
        wait_bytes(zgain, c_sem.at[0])


def flush(*refs):
    count = len(refs) // 2
    sems = refs[-1]
    copies = [
        pltpu.make_async_copy(refs[i], refs[count + i], sems.at[i]) for i in range(count)
    ]
    for copy in copies:
        copy.start()
    for copy in copies:
        copy.wait()


def per_device(sizes, query, key, value, out_grad, query_gain, key_gain, rel_bias):
    nz, ny, nx, nc = sizes
    vmem = pl.BlockSpec(memory_space=pltpu.VMEM)
    hbm = pl.BlockSpec(memory_space=pl.ANY)
    dma = pltpu.SemaphoreType.DMA
    regular = pltpu.SemaphoreType.REGULAR
    shapes = (((ROWS, LANES), bf16),) * 3 + (((1, HD), f32),) * 2 + ((rel_bias.shape, f32),)
    tile_rows, wide_rows = (ROWS, LANES), (TILES * WIDE, LANES)
    square = (ROWS, TILES * WIDE)
    outs = pl.pallas_call(
        functools.partial(body, sizes),
        out_shape=tuple(pltpu.VMEM(*s) for s in shapes),
        in_specs=[hbm] * 7,
        out_specs=(vmem,) * 6,
        scratch_shapes=[
            *[pltpu.VMEM((1, HD), f32)] * 2,
            pltpu.VMEM(rel_bias.shape, f32),
            *[pltpu.VMEM((TILES, 2 * TILE, LANES), bf16)] * 4,
            *[pltpu.VMEM((TILES, 2, WIDE), f32)] * 2,
            *[pltpu.VMEM(tile_rows, f32)] * 5,
            *[pltpu.VMEM(tile_rows, bf16)] * 3,
            *[pltpu.VMEM(wide_rows, bf16)] * 4,
            *[pltpu.VMEM((TILES, (TILES + 1) * TILE, WIDE), f32)] * 2,
            pltpu.VMEM((TILES, (TILES + 1) * TILE, WIDE), bf16),
            *[pltpu.VMEM(square, f32)] * 2,
            *[pltpu.VMEM(square, bf16)] * 3,
            pltpu.VMEM((ny, 4, LANES), f32),
            pltpu.VMEM((nc * nx * ny, 1, LANES), f32),
            pltpu.VMEM((1, LANES), f32),
            pltpu.VMEM((1, LANES), f32),
            pltpu.VMEM((nz, 4, LANES), f32),
            pltpu.VMEM((1, LANES), f32),
            pltpu.VMEM((nz, 1, LANES), f32),
            dma((6,)),
            dma((TILES + 1,)),
            dma((3,)),
            dma((2,)),
            dma((4,)),
            dma((2,)),
            dma((2,)),
            regular((7,)),
        ],
        compiler_params=pltpu.CompilerParams(collective_id=0, has_side_effects=True),
        name="segment_backward",
    )(query, key, value, out_grad, query_gain.reshape(1, HD), key_gain.reshape(1, HD), rel_bias)
    outs = pl.pallas_call(
        flush,
        out_shape=tuple(jax.ShapeDtypeStruct(*s) for s in shapes),
        in_specs=[vmem] * 6,
        out_specs=(hbm,) * 6,
        scratch_shapes=[dma((6,))],
        name="flush",
    )(*(pltpu.with_memory_space_constraint(o, pltpu.VMEM) for o in outs))
    return (*outs[:3], outs[3].reshape(HD), outs[4].reshape(HD), outs[5])


def solution(mesh):
    sizes = mesh_sizes(mesh)
    torus = Mesh(mesh.devices.reshape(sizes), ("z", "y", "x", "c"))
    return jax.shard_map(
        functools.partial(per_device, sizes),
        mesh=torus,
        in_specs=(P(SP, TP), P(SP, TP), P(SP, TP), P(SP, TP), P(), P(), P(TP, None)),
        out_specs=(P(SP, TP), P(SP, TP), P(SP, TP), P(), P(), P(TP, None)),
        check_vma=False,
    )


def mesh_sizes(mesh):
    return (16, 8, 4, 2)
```
